256 devices in a mesh: ep: 32 (over z, x), tp: 8 (over y, core).
Axes of the slice: x: 4, y: 4, z: 8, core: 2. Of those that a mesh axis runs over, the one named last changes fastest.
Arguments:
- stream: bfloat16 [512, 4096], P(None, 'ep'), may hold values from -6.5 to 6.5
- norm_gain: float32 [4096], P('ep'), may hold values from 0.1 to 1.9
- w_query: bfloat16 [4096, 2048], P('ep', 'tp'), may hold values from -0.09375 to 0.09375
- w_key: bfloat16 [4096, 1024], P('ep', 'tp'), may hold values from -0.09375 to 0.09375
- w_value: bfloat16 [4096, 1024], P('ep', 'tp'), may hold values from -0.09375 to 0.09375
- break_offset: float32 [16], P('tp'), may hold values from -10 to -2
- cache_keys: bfloat16 [512, 1024, 8, 128], P('ep', None, 'tp'), may hold values from -6 to 6
- cache_values: bfloat16 [512, 1024, 8, 128], P('ep', None, 'tp'), may hold values from -6 to 6
- lengths: int32 [512], P('ep'), may hold values from 128 to 1024
- w_output: bfloat16 [2048, 4096], P('tp', 'ep'), may hold values from -0.125 to 0.125
- head_gain: float32 [2048], P('tp'), may hold values from 0.1 to 1.9
- ffn_gain: float32 [4096], P('ep'), may hold values from 0.1 to 1.9
- route_experts: int32 [512, 2], replicated, may hold values from 0 to 31, all different within a row; in each aligned block of 512 rows (0 to 511, 512 to 1023, ...) at most 64 rows name the same one
- route_weights: float32 [512, 2], replicated, may hold values from 0.1 to 1
- expert_gate: bfloat16 [32, 4096, 1024], P('ep', None, 'tp'), may hold values from -0.09375 to 0.09375
- expert_up: bfloat16 [32, 4096, 1024], P('ep', None, 'tp'), may hold values from -0.09375 to 0.09375
- expert_down: bfloat16 [32, 1024, 4096], P('ep', 'tp'), may hold values from -0.1875 to 0.1875
- dense_gate: bfloat16 [4096, 4096], P('ep', 'tp'), may hold values from -0.09375 to 0.09375
- dense_up: bfloat16 [4096, 4096], P('ep', 'tp'), may hold values from -0.09375 to 0.09375
- dense_down: bfloat16 [4096, 4096], P('tp', 'ep'), may hold values from -0.09375 to 0.09375
- mix_gain: float32 [4096], P('ep'), may hold values from 0.1 to 1.9
Outputs:
- mixed_out: bfloat16 [512, 4096], P(None, 'ep')
- key_rows: bfloat16 [512, 1024], P('ep', 'tp')
- value_rows: bfloat16 [512, 1024], P('ep', 'tp')
The draws below stay inside these ranges and needn't reach their ends.
Inputs may be any that keep to these rules, and one draw needn't show every extreme that they name: `route_experts`: in the whole batch no expert is named by more than 64 pairs, a bound that some block reaches; the 2 experts of a token differ.
All inputs are finite; a program needn't handle non-finite values.
Results may differ from the reference program's by a relative error of at most 0.025.
Values may be sent and summed in bfloat16 or wider, within the bound.
A program may use at most 64 MiB of HBM per device.

```python
import math
import jax
import jax.numpy as jnp
import numpy as np
from jax import lax

D = 4096
HEADS = 16
KVH = 8
HD = 128
FF = 1024
FD = 4096
TOP_K = 2
LEN = 1024
SEQS = 512
EXPERTS = 32
CAP = 64
N_TP = 8


def draw_stream(key, part):
    columns = jnp.arange(D, dtype=jnp.float32) / D
    col_scale = 0.6 * jnp.power(3.0, columns)[None, :]
    base_draw = jnp.clip(jax.random.normal(key, (SEQS, D), jnp.float32), -3.3, 3.3)
    values = base_draw * col_scale
    return values.astype(jnp.bfloat16)


def draw_break_offset(key, part):
    centre = -jnp.log(jnp.float32(LEN))
    spread = jax.random.uniform(jax.random.fold_in(key, 7), (HEADS,), jnp.float32, -1.2, 0.8)
    return (centre + spread).astype(jnp.float32)


def plant(drawn, key, low, high):
    dims = drawn.shape
    place = [jax.random.randint(jax.random.fold_in(key, axis), (), 0, dims[axis]) for axis in range(len(dims))]
    drawn = drawn.at[tuple(place)].set(low)
    longest = dims.index(max(dims))
    place[longest] = (place[longest] + 1) % dims[longest]
    return drawn.at[tuple(place)].set(high)


def levels(rng, shape, split, smallest, top_value):
    def one(dim, blocks):
        steps = jax.random.uniform(jax.random.fold_in(jax.random.fold_in(rng, 6), dim), (blocks,), jnp.float32, smallest / len(split), top_value / len(split))
        return jnp.repeat(jnp.exp(steps), shape[dim] // blocks).reshape((-1,) + (1,) * (len(shape) - dim - 1))

    loudness = one(*split[0])
    for cut in split[1:]:
        loudness = loudness * one(*cut)
    return loudness


def assign_block(rng, own, number, rows, count, top, bound, lean):
    sequence = jax.random.permutation(rng, count)
    crowded, ordinary = portions_of(count, rows * top, bound, lean, True), portions_of(count, rows * top, bound, lean, False)
    places = jnp.arange(count)

    def named(tallies, offset_by):
        used = int((tallies > 0).sum())
        fixed = max(1, used // 4)
        moved = fixed + (places - fixed + offset_by * (used - fixed)) % max(1, count - fixed)
        return jnp.zeros((count,), jnp.int32).at[sequence[jnp.where(places < fixed, places, moved)]].set(jnp.asarray(tallies, jnp.int32))

    tallies = jnp.where(number % 4 == 0, named(crowded, number // 4), named(ordinary, number - number // 4 - 1))
    mixed = jax.random.permutation(jax.random.fold_in(own, 3), count)
    donor, sink = mixed[0:count // 2 * 2:2], mixed[1:count // 2 * 2:2]
    margin = jnp.minimum(tallies[donor] - 1, bound - tallies[sink]) // 2
    margin = jnp.where((donor == sequence[0]) | (sink == sequence[0]) | (tallies[sink] == 0), 0, jnp.maximum(margin, 0))
    moved = jax.random.randint(jax.random.fold_in(own, 4), (count // 2,), 0, 1 << 20) % (margin + 1)
    tallies = tallies.at[donor].add(-moved).at[sink].add(moved)
    members = jnp.searchsorted(jnp.cumsum(tallies), jnp.arange(rows * top), side="right").astype(jnp.int32)
    listing = members.reshape(top, rows).T
    listing = listing[jax.random.permutation(jax.random.fold_in(own, 1), rows)]
    offset_by = jax.random.randint(jax.random.fold_in(own, 2), (rows, 1), 0, top)
    return jnp.take_along_axis(listing, (jnp.arange(top)[None, :] + offset_by) % top, axis=1)


def portions_of(count, total, most, lean, full):
    portions = [(1 << 20) // math.isqrt(rank ** lean) + 1 for rank in range(1, count + 1)]
    largest = most if full else min(most, max(-(-total // count), total * portions[0] // sum(portions)))
    least = 1 if total - largest >= count - 1 else 0
    given, rest = [largest] + [least] * (count - 1), total - largest - least * (count - 1)
    while rest > 0:
        movable = [i for i in range(1, count) if given[i] < largest] or [i for i in range(1, count) if given[i] < most]
        pool, budget = sum([portions[i] for i in movable]), rest
        for i in movable:
            addition = min(most - given[i], max(1, budget * portions[i] // pool), rest)
            given[i] = given[i] + addition
            rest = rest - addition
    return np.array(given)


def normal_values(stream_key, extent, deviation, limit, pieces=(), kind=jnp.bfloat16):
    array = jax.random.normal(stream_key, extent, jnp.float32) * deviation
    if len(pieces) > 0:
        array = levels(stream_key, extent, pieces, -0.22, 0.18) * array
    return jnp.clip(array, min=-limit, max=limit).astype(kind)


def setup_inputs(seed: int = 0) -> dict:
    arg_keys = jax.random.split(jax.random.key(seed), 22)
    stream = draw_stream(jax.random.fold_in(arg_keys[21], 71), 0)
    norm_gain = jnp.clip(1.0 + 0.18 * jax.random.normal(arg_keys[1], (D,), jnp.float32), 0.1, 1.9)
    w_query = normal_values(arg_keys[2], (D, HEADS * HD), D ** -0.5, 0.09375, ((0, 32), (1, 8)))
    w_key = normal_values(arg_keys[3], (D, KVH * HD), D ** -0.5, 0.09375, ((0, 32), (1, 8)))
    w_value = normal_values(arg_keys[4], (D, KVH * HD), D ** -0.5, 0.09375, ((0, 32), (1, 8)))
    break_offset = draw_break_offset(jax.random.fold_in(arg_keys[21], 71), 0)
    cache_keys = normal_values(arg_keys[6], (SEQS, LEN, KVH, HD), 1.0, 6.0, ((0, 32), (2, 8)))
    cache_values = normal_values(arg_keys[7], (SEQS, LEN, KVH, HD), 1.0, 6.0, ((0, 32), (2, 8)))
    lengths = plant(jax.random.randint(arg_keys[8], (SEQS,), LEN // 8, LEN + 1), jax.random.fold_in(arg_keys[8], 1), LEN // 8, LEN).astype(jnp.int32)
    w_output = normal_values(arg_keys[9], (HEADS * HD, D), (HEADS * HD) ** -0.5, 0.125, ((0, 8), (1, 32)))
    head_gain = jnp.clip(1.0 + 0.18 * jax.random.normal(arg_keys[10], (HEADS * HD,), jnp.float32), 0.1, 1.9)
    ffn_gain = jnp.clip(1.0 + 0.18 * jax.random.normal(arg_keys[11], (D,), jnp.float32), 0.1, 1.9)
    route_experts_keys = jax.random.split(jax.random.fold_in(arg_keys[12], 1), SEQS // SEQS)
    route_experts_turns = jax.random.permutation(jax.random.fold_in(arg_keys[12], 3), SEQS // SEQS)
    route_experts = jax.vmap(lambda own, number: assign_block(jax.random.fold_in(arg_keys[12], 2), own, number, SEQS, EXPERTS, TOP_K, CAP, 2))(route_experts_keys, route_experts_turns).reshape((SEQS, TOP_K))
    route_weights = jnp.clip(jax.random.uniform(arg_keys[13], (SEQS, TOP_K), jnp.float32, 0.1, 1.0), 0.1, 1.0)
    expert_gate = normal_values(arg_keys[14], (EXPERTS, D, FF), D ** -0.5, 0.09375, ((0, 32), (2, 8)))
    expert_up = normal_values(arg_keys[15], (EXPERTS, D, FF), D ** -0.5, 0.09375, ((0, 32), (2, 8)))
    expert_down = normal_values(arg_keys[16], (EXPERTS, FF, D), FF ** -0.5, 0.1875, ((0, 32), (1, 8)))
    dense_gate = normal_values(arg_keys[17], (D, FD), D ** -0.5, 0.09375, ((0, 32), (1, 8)))
    dense_up = normal_values(arg_keys[18], (D, FD), D ** -0.5, 0.09375, ((0, 32), (1, 8)))
    dense_down = normal_values(arg_keys[19], (FD, D), FD ** -0.5, 0.09375, ((0, 8), (1, 32)))
    mix_gain = jnp.clip(1.0 + 0.18 * jax.random.normal(arg_keys[20], (D,), jnp.float32), 0.1, 1.9)
    return {"stream": stream, "norm_gain": norm_gain, "w_query": w_query, "w_key": w_key, "w_value": w_value, "break_offset": break_offset, "cache_keys": cache_keys, "cache_values": cache_values, "lengths": lengths, "w_output": w_output, "head_gain": head_gain, "ffn_gain": ffn_gain, "route_experts": route_experts, "route_weights": route_weights, "expert_gate": expert_gate, "expert_up": expert_up, "expert_down": expert_down, "dense_gate": dense_gate, "dense_up": dense_up, "dense_down": dense_down, "mix_gain": mix_gain}


EPSILON = 1e-06

def rms_rows(values, gain_vec):
    return values * lax.rsqrt(lax.optimization_barrier(jnp.mean(values * values, axis=1, keepdims=True)) + EPSILON) * gain_vec[None, :]

def narrow_sum(left_side, right_side):
    per_group = right_side.shape[0] // N_TP
    summed = jnp.zeros((left_side.shape[0], right_side.shape[1]), jnp.float32)
    for group_index in range(N_TP):
        partial_value = jnp.dot(left_side[:, group_index * per_group:(group_index + 1) * per_group], right_side[group_index * per_group:(group_index + 1) * per_group], preferred_element_type=jnp.float32)
        rounded = lax.optimization_barrier(partial_value.astype(jnp.bfloat16))
        summed = summed + rounded.astype(jnp.float32)
    return summed.astype(jnp.bfloat16)

def slot_table(route_experts, experts, capacity):
    chosen = route_experts.reshape(-1)
    onehot = (chosen[:, None] == jnp.arange(experts, dtype=jnp.int32)[None, :]).astype(jnp.int32)
    earlier = jnp.cumsum(onehot, axis=0) - onehot
    rank_in = lax.optimization_barrier(jnp.sum(earlier * onehot, axis=1)).astype(jnp.int32)
    slot_ids = (chosen * capacity + rank_in).astype(jnp.int32)
    owners = jnp.arange(chosen.shape[0], dtype=jnp.int32) // route_experts.shape[1]
    filled = jnp.full((experts * capacity,), route_experts.shape[0], jnp.int32).at[slot_ids].set(owners)
    return (slot_ids, filled)

def reference(stream, norm_gain, w_query, w_key, w_value, break_offset, cache_keys, cache_values, lengths, w_output, head_gain, ffn_gain, route_experts, route_weights, expert_gate, expert_up, expert_down, dense_gate, dense_up, dense_down, mix_gain):
    streamf = stream.astype(jnp.float32)
    normed = rms_rows(streamf, norm_gain).astype(jnp.bfloat16)
    queries = jnp.dot(normed, w_query, preferred_element_type=jnp.float32).astype(jnp.bfloat16)
    key_rows = jnp.dot(normed, w_key, preferred_element_type=jnp.float32).astype(jnp.bfloat16)
    value_rows = jnp.dot(normed, w_value, preferred_element_type=jnp.float32).astype(jnp.bfloat16)
    seq_total = stream.shape[0]
    heads = break_offset.shape[0]
    kv_heads = cache_keys.shape[2]
    head_dim = cache_keys.shape[3]
    group_size = heads // kv_heads
    offsets = break_offset.reshape(kv_heads, group_size)[:, :, None]
    gains = head_gain.reshape(kv_heads, group_size, head_dim)

    def attend(inputs):
        query_one, keys_one, values_one, length_one = inputs
        scores = jnp.einsum('kgd,lkd->kgl', query_one.astype(jnp.float32), keys_one.astype(jnp.float32))
        scores = scores * head_dim ** (-0.5) + offsets
        in_cache = (jnp.arange(keys_one.shape[0], dtype=jnp.int32) < length_one)[None, None, :]
        failed = jnp.where(in_cache, jax.nn.log_sigmoid(-scores), 0.0)
        later_sum = lax.cumsum(failed, axis=2, reverse=True) - failed
        weights = jnp.where(in_cache, jnp.exp(jax.nn.log_sigmoid(scores) + later_sum), 0.0).astype(jnp.bfloat16)
        attended = jnp.einsum('kgl,lkd->kgd', weights.astype(jnp.float32), values_one.astype(jnp.float32))
        normalized = attended * lax.rsqrt(lax.optimization_barrier(jnp.mean(attended * attended, axis=2, keepdims=True)) + EPSILON) * gains
        return normalized.astype(jnp.bfloat16).reshape(heads * head_dim)
    head_out = lax.map(attend, (queries.reshape(seq_total, kv_heads, group_size, head_dim), cache_keys, cache_values, lengths))
    attn_out = narrow_sum(head_out, w_output)
    residual = streamf + attn_out.astype(jnp.float32)
    normed_ffn = rms_rows(residual, ffn_gain).astype(jnp.bfloat16)
    gate_part = jnp.dot(normed_ffn, dense_gate, preferred_element_type=jnp.float32)
    up_part = jnp.dot(normed_ffn, dense_up, preferred_element_type=jnp.float32)
    dense_hidden = (jax.nn.silu(gate_part) * up_part).astype(jnp.bfloat16)
    dense_out = narrow_sum(dense_hidden, dense_down)
    experts = expert_gate.shape[0]
    slot_ids, filled = slot_table(route_experts, experts, CAP)
    padded = jnp.concatenate([normed_ffn, jnp.zeros((1, normed_ffn.shape[1]), jnp.bfloat16)], axis=0)
    expert_in = padded[filled].reshape(experts, CAP, normed_ffn.shape[1])

    def expert_one(inputs):
        rows_in, gate_one, up_one, down_one = inputs
        gate_val = jnp.dot(rows_in, gate_one, preferred_element_type=jnp.float32)
        up_val = jnp.dot(rows_in, up_one, preferred_element_type=jnp.float32)
        expert_hidden = (jax.nn.silu(gate_val) * up_val).astype(jnp.bfloat16)
        return narrow_sum(expert_hidden, down_one)
    expert_out = lax.map(expert_one, (expert_in, expert_gate, expert_up, expert_down))
    picked = expert_out.reshape(experts * CAP, -1)[slot_ids].reshape(seq_total, route_experts.shape[1], -1)
    shares = route_weights / lax.optimization_barrier(jnp.sum(route_weights, axis=1, keepdims=True))
    moe_out = lax.optimization_barrier(jnp.sum(picked.astype(jnp.float32) * shares[:, :, None], axis=1))
    mixed_out = (residual + moe_out + mix_gain[None, :] * dense_out.astype(jnp.float32)).astype(jnp.bfloat16)
    return (mixed_out, key_rows, value_rows)
```

```python
import functools

import jax
import jax.numpy as jnp
from jax import lax
from jax.experimental import pallas as pl
from jax.experimental.pallas import tpu as pltpu
from jax.sharding import PartitionSpec as P

EPSILON = 1e-06
NX, NZ, NT = 4, 8, 8
MODEL, HD, LEN, ROWS = 4096, 128, 1024, 16
F32, BF16 = jnp.float32, jnp.bfloat16
HIGH = lax.Precision.HIGHEST


def iota(shape, dim):
    return lax.broadcasted_iota(jnp.int32, shape, dim)


def front_kernel(
    stream, wq, wk, wv, ck, cv, wo, ngain, hgain, boff, lens,
    attn_out, key_rows, value_rows,
    strm, wqkv, kbuf, vbuf, ybuf, yrecv, ssq, ssqr, zbuf, zrecv, zsq, zsqr,
    wog, hall, obuf, orecv, abuf, agath,
    lsem, ssem,
    yx_sem, sx_sem, wo_sem, yz_sem, sz_sem, h_sem, o_sem, a_sem,
):
    e = lax.axis_index("ep")
    t = lax.axis_index("tp")
    z = lax.div(e, NX)
    x = lax.rem(e, NX)

    def at_x(d):
        return lax.rem(x + d, NX)

    def at_z(d):
        return lax.rem(z + d, NZ)

    def at_t(d):
        return lax.rem(t + d, NT)

    started = []

    def send(src, dst, rsem, dev_e, dev_t):
        copy = pltpu.make_async_remote_copy(
            src_ref=src, dst_ref=dst, send_sem=ssem.at[len(started)], recv_sem=rsem,
            device_id=(dev_e, dev_t), device_id_type=pl.DeviceIdType.MESH,
        )
        copy.start()
        started.append(copy)

    def arrived(dst, rsem):
        pltpu.make_async_copy(dst, dst, rsem).wait()

    local = []

    def load(src, dst):
        copy = pltpu.make_async_copy(src, dst, lsem.at[len(local)])
        copy.start()
        local.append(copy)
        return copy

    c_w = [load(wq, wqkv.at[:, 0:256]), load(wk, wqkv.at[:, 256:384]), load(wv, wqkv.at[:, 384:512])]
    c_s = [load(stream.at[:, xi], strm.at[xi]) for xi in range(NX)]

    barrier = pltpu.get_barrier_semaphore()
    peers = 0
    for dz in range(NZ):
        for dx in range(NX):
            if dz == 0 or dx == 0:
                if dz or dx:
                    pl.semaphore_signal(barrier, inc=1, device_id=(at_z(dz) * NX + at_x(dx), t), device_id_type=pl.DeviceIdType.MESH)
                    peers += 1
    for dt in range(1, NT):
        for dx in range(NX):
            pl.semaphore_signal(barrier, inc=1, device_id=(z * NX + at_x(dx), at_t(dt)), device_id_type=pl.DeviceIdType.MESH)
            peers += 1

    c_k = load(ck, kbuf)
    c_v = load(cv, vbuf)
    c_wo = load(wo, wog.at[x])

    for c in c_w + c_s:
        c.wait()
    gain = ngain[...]
    w = wqkv[...]
    for xi in range(NX):
        rows = strm[xi].reshape(NZ * ROWS, HD).astype(F32)
        ybuf[xi] = jnp.dot((rows * gain).astype(BF16), w, preferred_element_type=F32).astype(BF16)
        sums = jnp.sum((rows * rows).T, axis=0, keepdims=True)
        ssq[xi] = jnp.broadcast_to(sums, (8, HD))

    pl.semaphore_wait(barrier, peers)

    for d in (2, 1, 3):
        to = z * NX + at_x(d)
        send(ybuf.at[at_x(d)], yrecv.at[d - 1], yx_sem.at[d - 1], to, t)
        send(ssq.at[at_x(d)], ssqr.at[d - 1], sx_sem.at[d - 1], to, t)
    c_wo.wait()
    for d in (2, 1, 3):
        send(wog.at[x], wog.at[x], wo_sem.at[d - 1], z * NX + at_x(d), t)
    total = ybuf[x].astype(F32)
    sq = ssq[x]
    for d in (1, 3, 2):
        arrived(yrecv.at[d - 1], yx_sem.at[d - 1])
        arrived(ssqr.at[d - 1], sx_sem.at[d - 1])
        total = total + yrecv[d - 1].astype(F32)
        sq = sq + ssqr[d - 1]
    zbuf[...] = total.astype(BF16).reshape(NZ, ROWS, 512)
    zsq[...] = sq

    for d in (4, 3, 5, 2, 6, 1, 7):
        to = at_z(d) * NX + x
        send(zbuf.at[at_z(d)], zrecv.at[d - 1], yz_sem.at[d - 1], to, t)
        send(zsq, zsqr.at[d - 1], sz_sem.at[d - 1], to, t)
    qkv = zbuf[z].astype(F32)
    sq = zsq[...]
    for d in (1, 7, 2, 6, 3, 5, 4):
        arrived(zrecv.at[d - 1], yz_sem.at[d - 1])
        arrived(zsqr.at[d - 1], sz_sem.at[d - 1])
        qkv = qkv + zrecv[d - 1].astype(F32)
        sq = sq + zsqr[d - 1]
    lane = iota((ROWS, HD), 1)
    pick = lane == z * ROWS + iota((ROWS, HD), 0)
    mean = jnp.sum(jnp.where(pick, jnp.broadcast_to(sq[0:1], (ROWS, HD)), 0.0), axis=1, keepdims=True) / MODEL
    qkv = qkv * lax.rsqrt(mean + EPSILON)
    key_rows[...] = qkv[:, 256:384].astype(BF16)
    value_rows[...] = qkv[:, 384:512].astype(BF16)

    q = jnp.concatenate([qkv[:, 0:128], qkv[:, 128:256]], axis=0).astype(BF16).astype(F32)
    seq = lax.rem(iota((2 * ROWS, 1), 0), ROWS)
    c_k.wait()
    scores = jnp.zeros((2 * ROWS, LEN), F32)
    for p in range(ROWS // 2):
        keys = jnp.concatenate([kbuf[2 * p], kbuf[2 * p + 1]], axis=1)
        own = jnp.concatenate([jnp.where(seq == 2 * p, q, 0.0), jnp.where(seq == 2 * p + 1, q, 0.0)], axis=1)
        scores = scores + lax.dot_general(own.astype(BF16), keys, (((1,), (1,)), ((), ())), preferred_element_type=F32)
    first = iota((2 * ROWS, 1), 0) < ROWS
    length = jnp.zeros((2 * ROWS, 1), jnp.int32)
    for s in range(ROWS):
        length = jnp.where(seq == s, lens[s], length)
    scores = scores * HD ** (-0.5) + jnp.where(first, boff[0], boff[1])
    inside = iota((2 * ROWS, LEN), 1) < length
    tail = jnp.log1p(jnp.exp(-jnp.abs(scores)))
    failed = jnp.where(inside, -(jnp.maximum(scores, 0.0) + tail), 0.0)
    blocks = [failed[:, b * 128 : (b + 1) * 128] for b in range(LEN // 128)]
    later = (iota((128, 128), 0) > iota((128, 128), 1)).astype(F32)
    within = jnp.dot(jnp.concatenate(blocks, axis=0), later, precision=HIGH, preferred_element_type=F32)
    after = jnp.zeros((2 * ROWS, 1), F32)
    sums = []
    for b in reversed(range(LEN // 128)):
        sums.insert(0, within[b * 32 : (b + 1) * 32] + after)
        after = after + jnp.sum(blocks[b], axis=1, keepdims=True)
    later_sum = jnp.concatenate(sums, axis=1)
    weights = jnp.where(inside, jnp.exp(jnp.minimum(scores, 0.0) - tail + later_sum), 0.0).astype(BF16)
    c_v.wait()
    attended = jnp.zeros((2 * ROWS, HD), F32)
    for p in range(ROWS // 2):
        vals = jnp.concatenate([vbuf[2 * p], vbuf[2 * p + 1]], axis=1)
        both = jnp.dot(weights, vals, preferred_element_type=F32)
        attended = jnp.where(seq == 2 * p, both[:, 0:128], jnp.where(seq == 2 * p + 1, both[:, 128:256], attended))
    norm = lax.rsqrt(jnp.mean(attended * attended, axis=1, keepdims=True) + EPSILON)
    head = attended * norm * jnp.where(first, hgain[0:1], hgain[1:2])
    hall[z] = jnp.concatenate([head[:ROWS], head[ROWS:]], axis=1).astype(BF16)

    for d in (4, 3, 5, 2, 6, 1, 7):
        send(hall.at[z], hall.at[z], h_sem.at[d - 1], at_z(d) * NX + x, t)
    for d in (1, 2, 3):
        arrived(wog.at[at_x(NX - d)], wo_sem.at[d - 1])
    for d in (1, 7, 2, 6, 3, 5, 4):
        arrived(hall.at[at_z(NZ - d)], h_sem.at[d - 1])
    heads = hall[...].reshape(NZ * ROWS, 256)
    for xi in range(NX):
        part = jnp.dot(heads, wog[xi], preferred_element_type=F32)
        obuf[:, :, xi * 128 : (xi + 1) * 128] = part.astype(BF16).reshape(NZ, ROWS, 128)
    for d in (4, 5, 3, 2, 6, 7, 1):
        send(obuf.at[at_t(d)], orecv.at[d - 1], o_sem.at[d - 1], e, at_t(d))
    attn = obuf[t].astype(F32)
    for d in (1, 7, 2, 6, 3, 5, 4):
        arrived(orecv.at[d - 1], o_sem.at[d - 1])
        attn = attn + orecv[d - 1].astype(F32)
    attn = attn.astype(BF16)
    for xi in range(NX):
        abuf[xi] = attn[:, xi * 128 : (xi + 1) * 128]

    for dt in range(NT):
        for dx in range(NX):
            if dt or dx:
                send(abuf.at[at_x(dx)], agath.at[t, x], a_sem.at[dt * NX + dx], z * NX + at_x(dx), at_t(dt))
    agath[t, x] = abuf[x]
    for dt in range(NT):
        for dx in range(NX):
            if dt or dx:
                arrived(agath.at[at_t(NT - dt), at_x(NX - dx)], a_sem.at[dt * NX + dx])
    attn_out[...] = agath[...].reshape(512, 128)
    for copy in started:
        copy.wait_send()


def front(stream, norm_gain, wq, wk, wv, boff, ck, cv, lens, wo, hgain):
    any_spec = pl.BlockSpec(memory_space=pl.ANY)
    vm = pl.BlockSpec(memory_space=pltpu.VMEM)
    sm = pl.BlockSpec(memory_space=pltpu.SMEM)
    dma = pltpu.SemaphoreType.DMA
    return pl.pallas_call(
        front_kernel,
        name="front",
        out_shape=(
            jax.ShapeDtypeStruct((512, 128), BF16),
            jax.ShapeDtypeStruct((16, 128), BF16),
            jax.ShapeDtypeStruct((16, 128), BF16),
        ),
        in_specs=[any_spec] * 7 + [vm, vm, sm, sm],
        out_specs=(vm, vm, vm),
        scratch_shapes=[
            pltpu.VMEM((NX, NZ, ROWS, 128), BF16),
            pltpu.VMEM((128, 512), BF16),
            pltpu.VMEM((ROWS, LEN, 128), BF16),
            pltpu.VMEM((ROWS, LEN, 128), BF16),
            pltpu.VMEM((NX, 128, 512), BF16),
            pltpu.VMEM((NX - 1, 128, 512), BF16),
            pltpu.VMEM((NX, 8, 128), F32),
            pltpu.VMEM((NX - 1, 8, 128), F32),
            pltpu.VMEM((NZ, ROWS, 512), BF16),
            pltpu.VMEM((NZ - 1, ROWS, 512), BF16),
            pltpu.VMEM((8, 128), F32),
            pltpu.VMEM((NZ - 1, 8, 128), F32),
            pltpu.VMEM((NX, 256, 128), BF16),
            pltpu.VMEM((NZ, ROWS, 256), BF16),
            pltpu.VMEM((NZ, ROWS, 512), BF16),
            pltpu.VMEM((NT - 1, ROWS, 512), BF16),
            pltpu.VMEM((NX, ROWS, 128), BF16),
            pltpu.VMEM((NT, NX, ROWS, 128), BF16),
            dma((16,)),
            dma((96,)),
            dma((3,)), dma((3,)), dma((3,)), dma((7,)), dma((7,)), dma((7,)), dma((7,)), dma((32,)),
        ],
        compiler_params=pltpu.CompilerParams(collective_id=0, has_side_effects=True, vmem_limit_bytes=60 * 1024 * 1024),
    )(
        stream.reshape(NZ, NX, ROWS, 128), wq, wk, wv, ck.reshape(ROWS, LEN, 128), cv.reshape(ROWS, LEN, 128), wo,
        norm_gain.reshape(1, 128), hgain.reshape(2, 128), boff, lens,
    )


def sent_to_all(x, axis):
    size = lax.axis_size(axis)
    return lax.all_to_all(jnp.broadcast_to(x[None], (size, *x.shape)), axis, 0, 0, tiled=True)


def taken_together(x, axis):
    return sent_to_all(x, axis).sum(axis=0)


def split_up(x, dim, size):
    lengths = x.shape
    blocks = x.reshape(*lengths[:dim], size, lengths[dim] // size, *lengths[dim + 1 :])
    return jnp.moveaxis(blocks, dim, 0)


def sent_and_summed(x, axis, dim):
    blocks = split_up(x, dim, lax.axis_size(axis))
    arrived = lax.all_to_all(blocks, axis, split_axis=0, concat_axis=0, tiled=True)
    return arrived.astype(jnp.float32).sum(axis=0)


def joined_along(blocks, dim):
    blocks = jnp.moveaxis(blocks, 0, dim)
    lengths = blocks.shape
    return blocks.reshape(*lengths[:dim], lengths[dim] * lengths[dim + 1], *lengths[dim + 2 :])


def gather_directly(x, axis, dim):
    return joined_along(sent_to_all(x, axis), dim)


def of_everyone(x, axis):
    return sent_to_all(x, axis).astype(jnp.float32).sum(axis=0)


def rms_scale(values, gain_vec, model_width):
    squares = taken_together(jnp.sum(values * values, axis=1), "ep")
    return values * lax.rsqrt(squares / model_width + EPSILON)[:, None] * gain_vec[None, :]


def to_heads(normed, weights):
    return sent_and_summed(
        jnp.dot(normed, weights, preferred_element_type=jnp.float32).astype(jnp.bfloat16), "ep", 0
    )


def from_heads(values, weights):
    partial_value = jnp.dot(
        gather_directly(values, "ep", 0), weights, preferred_element_type=jnp.float32
    )
    return (
        of_everyone(partial_value.astype(jnp.bfloat16), "tp")
        .astype(jnp.float32)
        .astype(jnp.bfloat16)
    )


def expert_terms(inputs, gate_w, up_w, down_w):
    gate_val = jnp.einsum("ecd,edf->ecf", inputs, gate_w, preferred_element_type=jnp.float32)
    up_val = jnp.einsum("ecd,edf->ecf", inputs, up_w, preferred_element_type=jnp.float32)
    hidden = (jax.nn.silu(gate_val) * up_val).astype(jnp.bfloat16)
    return jnp.einsum("ecf,efd->ecd", hidden, down_w, preferred_element_type=jnp.float32)


def slot_table(route_experts, experts, capacity):
    chosen = route_experts.reshape(-1)
    onehot = (chosen[:, None] == jnp.arange(experts, dtype=jnp.int32)[None, :]).astype(jnp.int32)
    earlier = jnp.cumsum(onehot, axis=0) - onehot
    rank_in = jnp.sum(earlier * onehot, axis=1)
    slot_ids = chosen * capacity + rank_in
    owners = jnp.arange(chosen.shape[0], dtype=jnp.int32) // route_experts.shape[1]
    filled = (
        jnp.full((experts * capacity,), route_experts.shape[0], jnp.int32).at[slot_ids].set(owners)
    )
    return (slot_ids, filled)


def per_device(
    stream,
    norm_gain,
    w_query,
    w_key,
    w_value,
    break_offset,
    cache_keys,
    cache_values,
    lengths,
    w_output,
    head_gain,
    ffn_gain,
    route_experts,
    route_weights,
    expert_gate,
    expert_up,
    expert_down,
    dense_gate,
    dense_up,
    dense_down,
    mix_gain,
):
    model_width = stream.shape[1] * lax.axis_size("ep")
    block_width = stream.shape[1]
    seq_count = lengths.shape[0]
    streamf = stream.astype(jnp.float32)
    attn_out, key_rows, value_rows = front(
        stream, norm_gain, w_query, w_key, w_value, break_offset, cache_keys, cache_values, lengths, w_output, head_gain
    )
    residual = streamf + attn_out.astype(jnp.float32)
    normed_ffn = rms_scale(residual, ffn_gain, model_width).astype(jnp.bfloat16)
    dense_width = dense_gate.shape[1]
    gate_up = to_heads(normed_ffn, jnp.concatenate([dense_gate, dense_up], axis=1))
    dense_hidden = (jax.nn.silu(gate_up[:, :dense_width]) * gate_up[:, dense_width:]).astype(
        jnp.bfloat16
    )
    dense_out = from_heads(dense_hidden, dense_down)
    experts = expert_gate.shape[0] * lax.axis_size("ep")
    capacity = 2 * seq_count * route_experts.shape[1] // expert_gate.shape[0]
    slot_ids, filled = slot_table(route_experts, experts, capacity)
    padded = jnp.concatenate([normed_ffn, jnp.zeros((1, block_width), jnp.bfloat16)], axis=0)
    outgoing = padded[filled].reshape(experts, capacity, block_width)
    slot_share = capacity // lax.axis_size("tp")
    own_slots = lax.dynamic_slice_in_dim(outgoing, lax.axis_index("tp") * slot_share, slot_share, 1)
    arrived = lax.all_to_all(own_slots, "ep", split_axis=0, concat_axis=2, tiled=True)
    gathered = lax.all_gather(arrived, "tp", axis=1, tiled=True)
    partial_value = expert_terms(gathered, expert_gate, expert_up, expert_down)
    summed = sent_and_summed(partial_value.astype(jnp.bfloat16), "tp", 1).astype(jnp.bfloat16)
    came_back = lax.all_to_all(summed, "ep", split_axis=2, concat_axis=0, tiled=True)
    returned = gather_directly(came_back, "tp", 1)
    picked = returned.reshape(experts * capacity, block_width)[slot_ids]
    picked = picked.reshape(route_experts.shape[0], route_experts.shape[1], block_width).astype(
        jnp.float32
    )
    shares = route_weights / jnp.sum(route_weights, axis=1, keepdims=True)
    moe_out = jnp.sum(picked * shares[:, :, None], axis=1)
    mixed_out = (residual + moe_out + mix_gain[None, :] * dense_out.astype(jnp.float32)).astype(
        jnp.bfloat16
    )
    return (mixed_out, key_rows, value_rows)


def solution(mesh):
    in_specs = (
        P(None, "ep"),
        P("ep"),
        P("ep", "tp"),
        P("ep", "tp"),
        P("ep", "tp"),
        P("tp"),
        P("ep", None, "tp", None),
        P("ep", None, "tp", None),
        P("ep"),
        P("tp", "ep"),
        P("tp"),
        P("ep"),
        P(),
        P(),
        P("ep", None, "tp"),
        P("ep", None, "tp"),
        P("ep", "tp", None),
        P("ep", "tp"),
        P("ep", "tp"),
        P("tp", "ep"),
        P("ep"),
    )
    out_specs = (P(None, "ep"), P("ep", "tp"), P("ep", "tp"))
    return jax.shard_map(
        per_device, mesh=mesh, in_specs=in_specs, out_specs=out_specs, check_vma=False
    )
```

```python
import jax
import jax.numpy as jnp
from jax import lax
from jax.experimental import pallas as pl
from jax.experimental.pallas import tpu as pltpu
from jax.sharding import PartitionSpec as P

EPSILON = 1e-06
NX, NZ, NT = 4, 8, 8
MODEL, HD, LEN, ROWS, SEQS = 4096, 128, 1024, 16, 512
CAP, HALF = 64, 32
F32, BF16 = jnp.float32, jnp.bfloat16
HIGH = lax.Precision.HIGHEST
MESH = pl.DeviceIdType.MESH
FAR_FIRST = (4, 3, 5, 2, 6, 1, 7)
NEAR_FIRST = (1, 7, 2, 6, 3, 5, 4)


def iota(shape, dim):
    return lax.broadcasted_iota(jnp.int32, shape, dim)


def step_kernel(
    stream, wq, wk, wv, ck, cv, wo, eg, eu, ed, dg, du, dd,
    ngain, hgain, fgain, mgain, route, rweights, boff, lens,
    mixed, key_rows, value_rows,
    strm, wqkv, kbuf, vbuf, ybuf, yrecv, ssq, ssqr, zbuf, zrecv, zsq, zsqr,
    wog, hall, obuf, orecv, abuf, afin, sres, fgb, fgall, wgu, ddb, egb, eub, edb,
    pmat, ctm, rbuf, rall, gbuf, fsq, fsqr, gub, gurecv, dbuf, xe, hd,
    pown, pout, precv, rsum, rt, fbuf, frecv, mgath,
    lsem, ssem,
    yx_sem, sx_sem, wo_sem, wg_sem, wu_sem, sr_sem, fg_sem, yz_sem, sz_sem, h_sem, o_sem, af_sem, r_sem,
    fs_sem, gu_sem, d_sem, xe_sem, hz_sem, hx_sem, p_sem, rt_sem, f_sem, m_sem,
):
    e = lax.axis_index("ep")
    t = lax.axis_index("tp")
    z = lax.div(e, NX)
    x = lax.rem(e, NX)
    c = lax.rem(t, 2)
    partner = t + 1 - 2 * c

    def at_x(d):
        return lax.rem(x + d, NX)

    def at_z(d):
        return lax.rem(z + d, NZ)

    def at_t(d):
        return lax.rem(t + d, NT)

    started = []

    def send(src, dst, rsem, dev_e, dev_t):
        copy = pltpu.make_async_remote_copy(
            src_ref=src, dst_ref=dst, send_sem=ssem.at[len(started)], recv_sem=rsem,
            device_id=(dev_e, dev_t), device_id_type=MESH,
        )
        copy.start()
        started.append(copy)

    def arrived(dst, rsem):
        pltpu.make_async_copy(dst, dst, rsem).wait()

    loads = []

    def load(src, dst):
        copy = pltpu.make_async_copy(src, dst, lsem.at[len(loads)])
        copy.start()
        loads.append(copy)
        return copy

    def columns(ref, block):
        return ref.at[:, pl.ds(pl.multiple_of(block * 128, 128), 128)]

    c_w = [load(wq, wqkv.at[:, 0:256]), load(wk, wqkv.at[:, 256:384]), load(wv, wqkv.at[:, 384:512])]
    c_s = [load(stream.at[:, xi], strm.at[xi]) for xi in range(NX)]

    barrier = pltpu.get_barrier_semaphore()
    peers = 0
    for dt in range(NT):
        for dz in range(NZ):
            for dx in range(NX):
                if (dt == 0 and (dz or dx)) or (dt and dz == 0):
                    pl.semaphore_signal(barrier, inc=1, device_id=(at_z(dz) * NX + at_x(dx), at_t(dt)), device_id_type=MESH)
                    peers += 1

    c_wo = load(wo, wog.at[x])
    c_k = load(ck, kbuf)
    c_v = load(cv, vbuf)
    c_dg = load(columns(dg, x), wgu.at[x, :, 0:128])
    c_du = load(columns(du, x), wgu.at[x, :, 128:256])
    c_dd = load(dd, ddb)
    c_eg = load(eg, egb)
    c_eu = load(eu, eub)
    c_ed = [load(ed.at[:, zi * 512 : (zi + 1) * 512], edb.at[zi]) for zi in range(NZ)]

    for copy in c_w + c_s:
        copy.wait()
    gain = ngain[...]
    w = wqkv[...]
    for xi in range(NX):
        rows = strm[xi].reshape(NZ * ROWS, HD).astype(F32)
        ybuf[xi] = jnp.dot((rows * gain).astype(BF16), w, preferred_element_type=F32).astype(BF16)
        sums = jnp.sum((rows * rows).T, axis=0, keepdims=True)
        ssq[xi] = jnp.broadcast_to(sums, (8, HD))
    fgb[...] = jnp.broadcast_to(fgain[...], (8, HD))

    pl.semaphore_wait(barrier, peers)

    for d in (2, 1, 3):
        to = z * NX + at_x(d)
        send(ybuf.at[at_x(d)], yrecv.at[d - 1], yx_sem.at[d - 1], to, t)
        send(ssq.at[at_x(d)], ssqr.at[d - 1], sx_sem.at[d - 1], to, t)
    c_wo.wait()
    for d in (2, 1, 3):
        to = z * NX + at_x(d)
        send(wog.at[x], wog.at[x], wo_sem.at[d - 1], to, t)
        send(strm.at[at_x(d), t], sres.at[x], sr_sem.at[d - 1], to, t)
        send(fgb, fgall.at[x], fg_sem.at[d - 1], to, t)
        send(columns(dg, at_x(d)), wgu.at[x, :, 0:128], wg_sem.at[d - 1], to, t)
        send(columns(du, at_x(d)), wgu.at[x, :, 128:256], wu_sem.at[d - 1], to, t)
    sres[x] = strm[x, t]
    fgall[x] = fgb[...]

    names = [route[0:1], route[1:2]]
    expert = iota((32, SEQS), 0)
    chosen = (jnp.where(names[0] == expert, 1.0, 0.0) + jnp.where(names[1] == expert, 1.0, 0.0)).astype(BF16)
    before = jnp.where(iota((SEQS, SEQS), 0) < iota((SEQS, SEQS), 1), 1.0, 0.0).astype(BF16)
    earlier = jnp.dot(chosen, before, preferred_element_type=F32)
    slots = [
        n * CAP + jnp.sum(jnp.where(n == expert, earlier, 0.0), axis=0, keepdims=True).astype(jnp.int32) for n in names
    ]
    weight_sum = rweights[0:1] + rweights[1:2]
    shares = [rweights[0:1] / weight_sum, rweights[1:2] / weight_sum]
    for i in range(2):
        row = iota((128, SEQS), 0) + i * 128
        slot = lax.shift_right_logical(row, 5) * (NX * CAP) + (x * CAP + c * HALF) + (row & 31)
        pmat[i * 128 : (i + 1) * 128] = jnp.where((slots[0] == slot) | (slots[1] == slot), 1.0, 0.0).astype(BF16)
    for i in range(8):
        row = iota((128, SEQS), 0) + i * 128
        slot = lax.shift_right_logical(row, 5) * CAP + c * HALF + (row & 31)
        ctm[i * 128 : (i + 1) * 128] = jnp.where(
            slots[0] == slot, shares[0], jnp.where(slots[1] == slot, shares[1], 0.0)
        ).astype(BF16)

    total = ybuf[x].astype(F32)
    sq = ssq[x]
    for d in (1, 3, 2):
        arrived(yrecv.at[d - 1], yx_sem.at[d - 1])
        arrived(ssqr.at[d - 1], sx_sem.at[d - 1])
        total = total + yrecv[d - 1].astype(F32)
        sq = sq + ssqr[d - 1]
    zbuf[...] = total.astype(BF16).reshape(NZ, ROWS, 512)
    zsq[...] = sq

    for d in FAR_FIRST:
        to = at_z(d) * NX + x
        send(zbuf.at[at_z(d)], zrecv.at[d - 1], yz_sem.at[d - 1], to, t)
        send(zsq, zsqr.at[d - 1], sz_sem.at[d - 1], to, t)
    qkv = zbuf[z].astype(F32)
    sq = zsq[...]
    for d in NEAR_FIRST:
        arrived(zrecv.at[d - 1], yz_sem.at[d - 1])
        arrived(zsqr.at[d - 1], sz_sem.at[d - 1])
        qkv = qkv + zrecv[d - 1].astype(F32)
        sq = sq + zsqr[d - 1]
    lane = iota((ROWS, HD), 1)
    pick = lane == z * ROWS + iota((ROWS, HD), 0)
    mean = jnp.sum(jnp.where(pick, jnp.broadcast_to(sq[0:1], (ROWS, HD)), 0.0), axis=1, keepdims=True) / MODEL
    qkv = qkv * lax.rsqrt(mean + EPSILON)
    key_rows[...] = qkv[:, 256:384].astype(BF16)
    value_rows[...] = qkv[:, 384:512].astype(BF16)

    q = jnp.concatenate([qkv[:, 0:128], qkv[:, 128:256]], axis=0).astype(BF16).astype(F32)
    seq = lax.rem(iota((2 * ROWS, 1), 0), ROWS)
    c_k.wait()
    scores = jnp.zeros((2 * ROWS, LEN), F32)
    for p in range(ROWS // 2):
        keys = jnp.concatenate([kbuf[2 * p], kbuf[2 * p + 1]], axis=1)
        own = jnp.concatenate([jnp.where(seq == 2 * p, q, 0.0), jnp.where(seq == 2 * p + 1, q, 0.0)], axis=1)
        scores = scores + lax.dot_general(own.astype(BF16), keys, (((1,), (1,)), ((), ())), preferred_element_type=F32)
    first = iota((2 * ROWS, 1), 0) < ROWS
    length = jnp.zeros((2 * ROWS, 1), jnp.int32)
    for s in range(ROWS):
        length = jnp.where(seq == s, lens[s], length)
    scores = scores * HD ** (-0.5) + jnp.where(first, boff[0], boff[1])
    inside = iota((2 * ROWS, LEN), 1) < length
    tail = jnp.log1p(jnp.exp(-jnp.abs(scores)))
    failed = jnp.where(inside, -(jnp.maximum(scores, 0.0) + tail), 0.0)
    blocks = [failed[:, b * 128 : (b + 1) * 128] for b in range(LEN // 128)]
    later = (iota((128, 128), 0) > iota((128, 128), 1)).astype(F32)
    within = jnp.dot(jnp.concatenate(blocks, axis=0), later, precision=HIGH, preferred_element_type=F32)
    after = jnp.zeros((2 * ROWS, 1), F32)
    sums = []
    for b in reversed(range(LEN // 128)):
        sums.insert(0, within[b * 32 : (b + 1) * 32] + after)
        after = after + jnp.sum(blocks[b], axis=1, keepdims=True)
    later_sum = jnp.concatenate(sums, axis=1)
    weights = jnp.where(inside, jnp.exp(jnp.minimum(scores, 0.0) - tail + later_sum), 0.0).astype(BF16)
    c_v.wait()
    attended = jnp.zeros((2 * ROWS, HD), F32)
    for p in range(ROWS // 2):
        vals = jnp.concatenate([vbuf[2 * p], vbuf[2 * p + 1]], axis=1)
        both = jnp.dot(weights, vals, preferred_element_type=F32)
        attended = jnp.where(seq == 2 * p, both[:, 0:128], jnp.where(seq == 2 * p + 1, both[:, 128:256], attended))
    norm = lax.rsqrt(jnp.mean(attended * attended, axis=1, keepdims=True) + EPSILON)
    head = attended * norm * jnp.where(first, hgain[0:1], hgain[1:2])
    hall[z] = jnp.concatenate([head[:ROWS], head[ROWS:]], axis=1).astype(BF16)

    for d in FAR_FIRST:
        send(hall.at[z], hall.at[z], h_sem.at[d - 1], at_z(d) * NX + x, t)
    for d in (1, 2, 3):
        arrived(wog.at[at_x(NX - d)], wo_sem.at[d - 1])
        arrived(sres.at[at_x(NX - d)], sr_sem.at[d - 1])
        arrived(fgall.at[at_x(NX - d)], fg_sem.at[d - 1])
        arrived(wgu.at[at_x(NX - d), :, 0:128], wg_sem.at[d - 1])
        arrived(wgu.at[at_x(NX - d), :, 128:256], wu_sem.at[d - 1])
    c_dg.wait()
    c_du.wait()
    for d in NEAR_FIRST:
        arrived(hall.at[at_z(NZ - d)], h_sem.at[d - 1])
    heads = hall[...].reshape(NZ * ROWS, 256)
    for xi in range(NX):
        part = jnp.dot(heads, wog[xi], preferred_element_type=F32)
        obuf[:, :, xi * 128 : (xi + 1) * 128] = part.astype(BF16).reshape(NZ, ROWS, 128)
    for d in (4, 5, 3, 2, 6, 7, 1):
        send(obuf.at[at_t(d)], orecv.at[d - 1], o_sem.at[d - 1], e, at_t(d))
    attn = obuf[t].astype(F32)
    for d in NEAR_FIRST:
        arrived(orecv.at[d - 1], o_sem.at[d - 1])
        attn = attn + orecv[d - 1].astype(F32)
    attn = attn.astype(BF16)
    rbuf[...] = (attn.astype(F32) + jnp.concatenate([sres[xi].astype(F32) for xi in range(NX)], axis=1)).astype(BF16)
    for xi in range(NX):
        abuf[xi] = attn[:, xi * 128 : (xi + 1) * 128]

    for dt in (4, 5, 3, 2, 6, 7, 1, 0):
        for dx in (2, 1, 3, 0):
            if dt or dx:
                send(rbuf, rall.at[t, x], r_sem.at[dt * NX + dx], z * NX + at_x(dx), at_t(dt))
    for d in (2, 1, 3):
        send(abuf.at[at_x(d)], afin.at[x], af_sem.at[d - 1], z * NX + at_x(d), t)
    rall[t, x] = rbuf[...]
    afin[x] = abuf[x]
    for dt in range(NT):
        for dx in range(NX):
            if dt or dx:
                arrived(rall.at[at_t(NT - dt), at_x(NX - dx)], r_sem.at[dt * NX + dx])
    gains = jnp.concatenate([fgall[xi][0:1] for xi in range(NX)], axis=1)
    square_rows = []
    for i in range(4):
        rows = rall[2 * i : 2 * i + 2].reshape(128, 512).astype(F32)
        gbuf[i * 128 : (i + 1) * 128] = (rows * gains).astype(BF16)
        squares = rows * rows
        squares = squares[:, 0:128] + squares[:, 128:256] + squares[:, 256:384] + squares[:, 384:512]
        square_rows.append(jnp.sum(squares.T, axis=0, keepdims=True))
    fsq[...] = jnp.concatenate(square_rows + [jnp.zeros((4, 128), F32)], axis=0)
    dispatched = jnp.dot(pmat[...], gbuf[...], preferred_element_type=F32)
    dbuf[...] = dispatched.astype(BF16).reshape(NZ, HALF, 512)
    for d in FAR_FIRST:
        to = at_z(d) * NX + x
        send(dbuf.at[at_z(d)], xe.at[c, z], d_sem.at[d - 1], to, t)
        send(fsq, fsqr.at[d - 1], fs_sem.at[d - 1], to, t)
    xe[c, z] = dbuf[z]
    wide = wgu[...].reshape(512, 256)
    for i in range(4):
        part = jnp.dot(gbuf[i * 128 : (i + 1) * 128], wide, preferred_element_type=F32)
        gub[2 * i : 2 * i + 2] = part.astype(BF16).reshape(2, 64, 256)
    for d in FAR_FIRST:
        send(gub.at[at_z(d)], gurecv.at[d - 1], gu_sem.at[d - 1], at_z(d) * NX + x, t)

    send(xe.at[c, z], xe.at[c, z], xe_sem.at[0], e, partner)
    for d in NEAR_FIRST:
        arrived(xe.at[c, at_z(NZ - d)], d_sem.at[d - 1])
        send(xe.at[c, at_z(NZ - d)], xe.at[c, at_z(NZ - d)], xe_sem.at[d], e, partner)
    sq = fsq[...]
    for d in NEAR_FIRST:
        arrived(fsqr.at[d - 1], fs_sem.at[d - 1])
        sq = sq + fsqr[d - 1]
    inverse = lax.rsqrt(sq / MODEL + EPSILON)
    inverse = jnp.concatenate([inverse[i : i + 1] for i in range(4)], axis=1)
    slot = iota((CAP, SEQS), 0) + e * CAP
    mine = (slots[0] == slot) | (slots[1] == slot)
    slot_scale = jnp.sum(jnp.where(mine, jnp.broadcast_to(inverse, (CAP, SEQS)), 0.0), axis=1, keepdims=True)
    own_row = iota((64, SEQS), 1) == iota((64, SEQS), 0) + z * 64
    row_scale = jnp.sum(jnp.where(own_row, jnp.broadcast_to(inverse, (64, SEQS)), 0.0), axis=1, keepdims=True)
    c_eg.wait()
    c_eu.wait()
    acc = jnp.zeros((CAP, 256), F32)
    for d in (0,) + NEAR_FIRST:
        zs = at_z(NZ - d)
        arrived(xe.at[1 - c, zs], xe_sem.at[d])
        rows = jnp.concatenate([xe[0, zs], xe[1, zs]], axis=0)
        both = jnp.concatenate([egb[zs], eub[zs]], axis=1)
        acc = acc + jnp.dot(rows, both, preferred_element_type=F32)
    acc = acc * slot_scale
    gate = acc[:, 0:128]
    hidden = (gate / (1.0 + jnp.exp(-gate)) * acc[:, 128:256]).astype(BF16)
    for copy in c_ed:
        copy.wait()
    for k, d in enumerate(FAR_FIRST + (0,)):
        zi = at_z(d)
        part = jnp.dot(hidden, edb[zi], preferred_element_type=F32)
        kept = jnp.where(c == 0, part[:HALF], part[HALF:]).astype(BF16)
        given = jnp.where(c == 0, part[HALF:], part[:HALF]).astype(BF16)
        for xi in range(NX):
            pown[zi, xi] = kept[:, xi * 128 : (xi + 1) * 128]
            pout[zi, xi] = given[:, xi * 128 : (xi + 1) * 128]
        send(pout.at[zi], precv.at[zi], p_sem.at[k], e, partner)

    gu = gub[z].astype(F32)
    for d in NEAR_FIRST:
        arrived(gurecv.at[d - 1], gu_sem.at[d - 1])
        gu = gu + gurecv[d - 1].astype(F32)
    gu = gu * row_scale
    gate = gu[:, 0:128]
    hd[x, z] = (gate / (1.0 + jnp.exp(-gate)) * gu[:, 128:256]).astype(BF16)
    for d in FAR_FIRST:
        send(hd.at[x, z], hd.at[x, z], hz_sem.at[d - 1], at_z(d) * NX + x, t)

    for k, d in enumerate(FAR_FIRST + (0,)):
        zi = at_z(d)
        arrived(precv.at[zi], p_sem.at[k])
        rsum[zi] = (pown[zi].astype(F32) + precv[zi].astype(F32)).astype(BF16)
        for dx in (2, 1, 3, 0):
            if d or dx:
                send(rsum.at[zi, at_x(dx)], rt.at[e], rt_sem.at[d * NX + dx], zi * NX + at_x(dx), t)
    rt[e] = rsum[z, x]

    for dx in (2, 1, 3):
        send(hd.at[x, z], hd.at[x, z], hx_sem.at[dx - 1], z * NX + at_x(dx), t)
    for d in NEAR_FIRST:
        zs = at_z(NZ - d)
        arrived(hd.at[x, zs], hz_sem.at[d - 1])
        for dx in (2, 1, 3):
            send(hd.at[x, zs], hd.at[x, zs], hx_sem.at[d * 3 + dx - 1], z * NX + at_x(dx), t)

    for d in range(NZ):
        for dx in range(NX):
            if d or dx:
                arrived(rt.at[at_z(NZ - d) * NX + at_x(NX - dx)], rt_sem.at[d * NX + dx])
    moe = lax.dot_general(ctm[...], rt[...].reshape(1024, 128), (((0,), (0,)), ((), ())), preferred_element_type=F32)
    for d in (0,) + NEAR_FIRST:
        for dx in (1, 3, 2):
            arrived(hd.at[at_x(NX - dx), at_z(NZ - d)], hx_sem.at[d * 3 + dx - 1])
    c_dd.wait()
    dense = jnp.zeros((SEQS, 128), F32)
    for xi in range(NX):
        dense = dense + jnp.dot(hd[xi].reshape(SEQS, 128), ddb[xi * 128 : (xi + 1) * 128], preferred_element_type=F32)
    fbuf[...] = (moe + mgain[...] * dense).astype(BF16).reshape(NT, 64, 128)

    for d in (4, 5, 3, 2, 6, 7, 1):
        send(fbuf.at[at_t(d)], frecv.at[d - 1], f_sem.at[d - 1], e, at_t(d))
    for d in (1, 2, 3):
        arrived(afin.at[at_x(NX - d)], af_sem.at[d - 1])
    out = jnp.concatenate([strm[xi, t].astype(F32) + afin[xi].astype(F32) for xi in range(NX)], axis=0)
    out = out + fbuf[t].astype(F32)
    for d in NEAR_FIRST:
        arrived(frecv.at[d - 1], f_sem.at[d - 1])
        out = out + frecv[d - 1].astype(F32)
    mgath[t] = out.astype(BF16)
    for d in (4, 5, 3, 2, 6, 7, 1):
        send(mgath.at[t], mgath.at[t], m_sem.at[d - 1], e, at_t(d))
    for d in NEAR_FIRST:
        arrived(mgath.at[at_t(NT - d)], m_sem.at[d - 1])
    mixed[...] = mgath[...].reshape(SEQS, 128)
    for copy in started:
        copy.wait_send()


def per_device(
    stream, norm_gain, w_query, w_key, w_value, break_offset, cache_keys, cache_values, lengths, w_output, head_gain,
    ffn_gain, route_experts, route_weights, expert_gate, expert_up, expert_down, dense_gate, dense_up, dense_down, mix_gain,
):
    any_spec = pl.BlockSpec(memory_space=pl.ANY)
    vm = pl.BlockSpec(memory_space=pltpu.VMEM)
    sm = pl.BlockSpec(memory_space=pltpu.SMEM)
    dma = pltpu.SemaphoreType.DMA

    def b(*shape):
        return pltpu.VMEM(shape, BF16)

    def f(*shape):
        return pltpu.VMEM(shape, F32)

    scratch = dict(
        strm=b(NX, NZ, ROWS, 128), wqkv=b(128, 512), kbuf=b(ROWS, LEN, 128), vbuf=b(ROWS, LEN, 128),
        ybuf=b(NX, 128, 512), yrecv=b(NX - 1, 128, 512), ssq=f(NX, 8, 128), ssqr=f(NX - 1, 8, 128),
        zbuf=b(NZ, ROWS, 512), zrecv=b(NZ - 1, ROWS, 512), zsq=f(8, 128), zsqr=f(NZ - 1, 8, 128),
        wog=b(NX, 256, 128), hall=b(NZ, ROWS, 256), obuf=b(NZ, ROWS, 512), orecv=b(NT - 1, ROWS, 512),
        abuf=b(NX, ROWS, 128), afin=b(NX, ROWS, 128), sres=b(NX, ROWS, 128), fgb=f(8, 128), fgall=f(NX, 8, 128),
        wgu=b(NX, 128, 256), ddb=b(512, 128), egb=b(NZ, 512, 128), eub=b(NZ, 512, 128), edb=b(NZ, 128, 512),
        pmat=b(256, SEQS), ctm=b(1024, SEQS), rbuf=b(ROWS, 512), rall=b(NT, NX, ROWS, 512), gbuf=b(SEQS, 512),
        fsq=f(8, 128), fsqr=f(NZ - 1, 8, 128), gub=b(NZ, 64, 256), gurecv=b(NZ - 1, 64, 256),
        dbuf=b(NZ, HALF, 512), xe=b(2, NZ, HALF, 512), hd=b(NX, NZ, 64, 128),
        pown=b(NZ, NX, HALF, 128), pout=b(NZ, NX, HALF, 128), precv=b(NZ, NX, HALF, 128), rsum=b(NZ, NX, HALF, 128),
        rt=b(32, HALF, 128), fbuf=b(NT, 64, 128), frecv=b(NT - 1, 64, 128), mgath=b(NT, 64, 128),
        lsem=dma((24,)), ssem=dma((208,)),
        yx_sem=dma((3,)), sx_sem=dma((3,)), wo_sem=dma((3,)), wg_sem=dma((3,)), wu_sem=dma((3,)), sr_sem=dma((3,)),
        fg_sem=dma((3,)), yz_sem=dma((7,)), sz_sem=dma((7,)), h_sem=dma((7,)), o_sem=dma((7,)), af_sem=dma((3,)),
        r_sem=dma((32,)), fs_sem=dma((7,)), gu_sem=dma((7,)), d_sem=dma((7,)), xe_sem=dma((8,)), hz_sem=dma((7,)),
        hx_sem=dma((24,)), p_sem=dma((8,)), rt_sem=dma((32,)), f_sem=dma((7,)), m_sem=dma((7,)),
    )
    return pl.pallas_call(
        step_kernel,
        name="step",
        out_shape=(
            jax.ShapeDtypeStruct((SEQS, 128), BF16),
            jax.ShapeDtypeStruct((ROWS, 128), BF16),
            jax.ShapeDtypeStruct((ROWS, 128), BF16),
        ),
        in_specs=[any_spec] * 13 + [vm] * 6 + [sm] * 2,
        out_specs=(vm, vm, vm),
        scratch_shapes=list(scratch.values()),
        compiler_params=pltpu.CompilerParams(collective_id=0, has_side_effects=True, vmem_limit_bytes=60 * 1024 * 1024),
    )(
        stream.reshape(NZ, NX, ROWS, 128), w_query, w_key, w_value,
        cache_keys.reshape(ROWS, LEN, 128), cache_values.reshape(ROWS, LEN, 128), w_output,
        expert_gate.reshape(NZ, 512, 128), expert_up.reshape(NZ, 512, 128), expert_down.reshape(128, MODEL),
        dense_gate, dense_up, dense_down,
        norm_gain.reshape(1, 128), head_gain.reshape(2, 128), ffn_gain.reshape(1, 128), mix_gain.reshape(1, 128),
        route_experts.T, route_weights.T, break_offset, lengths,
    )


def solution(mesh):
    in_specs = (
        P(None, "ep"),
        P("ep"),
        P("ep", "tp"),
        P("ep", "tp"),
        P("ep", "tp"),
        P("tp"),
        P("ep", None, "tp", None),
        P("ep", None, "tp", None),
        P("ep"),
        P("tp", "ep"),
        P("tp"),
        P("ep"),
        P(),
        P(),
        P("ep", None, "tp"),
        P("ep", None, "tp"),
        P("ep", "tp", None),
        P("ep", "tp"),
        P("ep", "tp"),
        P("tp", "ep"),
        P("ep"),
    )
    out_specs = (P(None, "ep"), P("ep", "tp"), P("ep", "tp"))
    return jax.shard_map(
        per_device, mesh=mesh, in_specs=in_specs, out_specs=out_specs, check_vma=False
    )
```

```python
import jax
import jax.numpy as jnp
from jax import lax
from jax.experimental import pallas as pl
from jax.experimental.pallas import tpu as pltpu
from jax.sharding import PartitionSpec as P

EPSILON = 1e-06
NX, NZ, NT = 4, 8, 8
MODEL, HD, LEN, ROWS, SEQS = 4096, 128, 1024, 16, 512
CAP, HALF = 64, 32
F32, BF16 = jnp.float32, jnp.bfloat16
HIGH = lax.Precision.HIGHEST
MESH = pl.DeviceIdType.MESH
FAR_FIRST = (4, 3, 5, 2, 6, 1, 7)
NEAR_FIRST = (1, 7, 2, 6, 3, 5, 4)


def iota(shape, dim):
    return lax.broadcasted_iota(jnp.int32, shape, dim)


def step_kernel(
    stream, wq, wk, wv, ck, cv, wo, eg, eu, ed, dg, du, dd,
    ngain_hbm, hgain_hbm, fgain_hbm, mgain_hbm, route_hbm, rweights_hbm, boff_hbm, lens_hbm,
    mixed, key_rows, value_rows,
    ngain, hgain, fgain, mgain, route, rweights, boff, lens,
    strm, wqkv, kbuf, vbuf, xgain, yq, yqr, yk, ykr, ssq, ssqr, zq, zqr, zk, zkr, zsq, zsqr,
    wog, hall, obuf, orecv, sres, fgb, fgall, wgu, ddb, egb, eub, edb,
    pmat, ctm, rbuf, rall, gbuf, fsq, fsqr, gub, gurecv, dbuf, xe, hd,
    pown, pout, precv, rsum, rt, fbuf, fpair, fhalf, frecv, mgath,
    lsem, ssem, ring_sem,
    yq_sem, yk_sem, sx_sem, wo_sem, wg_sem, wu_sem, sr_sem, fg_sem, zq_sem, zk_sem, sz_sem, h_sem, o_sem, r_sem, rf_sem,
    fs_sem, gu_sem, d_sem, xe_sem, hz_sem, hx_sem, p_sem, rt_sem, f_sem, m_sem,
):
    e = lax.axis_index("ep")
    t = lax.axis_index("tp")
    z = lax.div(e, NX)
    x = lax.rem(e, NX)
    c = lax.rem(t, 2)
    partner = t + 1 - 2 * c

    def at_x(d):
        return lax.rem(x + d, NX)

    def at_z(d):
        return lax.rem(z + d, NZ)

    def at_t(d):
        return lax.rem(t + d, NT)

    started = []

    def send(src, dst, rsem, dev_e, dev_t):
        copy = pltpu.make_async_remote_copy(
            src_ref=src, dst_ref=dst, send_sem=ssem.at[len(started)], recv_sem=rsem,
            device_id=(dev_e, dev_t), device_id_type=MESH,
        )
        copy.start()
        started.append(copy)

    def arrived(dst, rsem):
        pltpu.make_async_copy(dst, dst, rsem).wait()

    loads = []

    def load(src, dst):
        copy = pltpu.make_async_copy(src, dst, lsem.at[len(loads)])
        copy.start()
        loads.append(copy)
        return copy

    def columns(ref, block):
        return ref.at[:, pl.ds(pl.multiple_of(block * 128, 128), 128)]

    def signal(sem, dev_e, dev_t):
        pl.semaphore_signal(sem, inc=1, device_id=(dev_e, dev_t), device_id_type=MESH)

    barrier = pltpu.get_barrier_semaphore()
    for d in (1, NZ - 1):
        signal(barrier, at_z(d) * NX + x, t)
    for d in range(1, NX):
        signal(barrier, z * NX + at_x(d), t)
    for d in range(1, NT):
        signal(barrier, e, at_t(d))

    c_s = [load(stream.at[:, xi], strm.at[xi]) for xi in range(NX)]
    c_w = [load(ngain_hbm, ngain), load(wq, wqkv.at[:, 0:256]), load(wk, wqkv.at[:, 256:384]), load(wv, wqkv.at[:, 384:512])]
    c_route = [load(route_hbm, route), load(rweights_hbm, rweights)]
    c_small = [load(hgain_hbm, hgain), load(mgain_hbm, mgain), load(boff_hbm, boff), load(lens_hbm, lens)]
    c_fg = load(fgain_hbm, fgain)
    c_wo = load(wo, wog.at[x])
    c_k = load(ck, kbuf)
    c_v = load(cv, vbuf)
    c_dg = load(columns(dg, x), wgu.at[x, :, 0:128])
    c_du = load(columns(du, x), wgu.at[x, :, 128:256])
    c_dd = load(dd, ddb)
    c_eg = load(eg, egb)
    c_eu = load(eu, eub)
    c_ed = [load(ed.at[:, zi * 512 : (zi + 1) * 512], edb.at[zi]) for zi in range(NZ)]

    for copy in c_s + c_w:
        copy.wait()
    gain = ngain[...]
    w = wqkv[...]
    for xi in range(NX):
        rows = strm[xi].reshape(NZ * ROWS, HD).astype(F32)
        scaled = (rows * gain).astype(BF16)
        xgain[xi] = scaled
        yq[xi] = jnp.dot(scaled, w[:, 0:256], preferred_element_type=F32).astype(BF16).reshape(NZ, ROWS, 256)
        sums = jnp.sum((rows * rows).T, axis=0, keepdims=True)
        ssq[xi] = jnp.broadcast_to(sums, (8, HD))
    c_fg.wait()
    fgb[...] = jnp.broadcast_to(fgain[...], (8, HD))

    pl.semaphore_wait(barrier, 2 + NX - 1 + NT - 1)

    for d in (2, 1, 3):
        send(ssq.at[at_x(d)], ssqr.at[d - 1], sx_sem.at[d - 1], z * NX + at_x(d), t)
    for k in FAR_FIRST + (0,):
        for d in (2, 1, 3):
            send(yq.at[at_x(d), at_z(k)], yqr.at[d - 1, k], yq_sem.at[k * 3 + d - 1], z * NX + at_x(d), t)
    signal(ring_sem.at[0], at_z(1) * NX + x, t)
    signal(ring_sem.at[1], at_z(7) * NX + x, t)
    c_wo.wait()
    for d in (2, 1, 3):
        to = z * NX + at_x(d)
        send(wog.at[x], wog.at[x], wo_sem.at[d - 1], to, t)
        send(strm.at[at_x(d), t], sres.at[x], sr_sem.at[d - 1], to, t)
        send(fgb, fgall.at[x], fg_sem.at[d - 1], to, t)
    sres[x] = strm[x, t]
    fgall[x] = fgb[...]
    pl.semaphore_wait(ring_sem.at[0], 1)
    pl.semaphore_wait(ring_sem.at[1], 1)
    signal(ring_sem.at[2], at_z(2) * NX + x, t)
    signal(ring_sem.at[3], at_z(6) * NX + x, t)
    for xi in range(NX):
        yk[xi] = jnp.dot(xgain[xi], w[:, 256:512], preferred_element_type=F32).astype(BF16).reshape(NZ, ROWS, 256)
    for d in (2, 1, 3):
        send(yk.at[at_x(d)], ykr.at[d - 1], yk_sem.at[d - 1], z * NX + at_x(d), t)
    for d in (2, 1, 3):
        to = z * NX + at_x(d)
        send(columns(dg, at_x(d)), wgu.at[x, :, 0:128], wg_sem.at[d - 1], to, t)
        send(columns(du, at_x(d)), wgu.at[x, :, 128:256], wu_sem.at[d - 1], to, t)
    pl.semaphore_wait(ring_sem.at[2], 1)
    pl.semaphore_wait(ring_sem.at[3], 1)

    sq = ssq[x]
    for d in (1, 3, 2):
        arrived(ssqr.at[d - 1], sx_sem.at[d - 1])
        sq = sq + ssqr[d - 1]
    zsq[...] = sq
    for d in FAR_FIRST:
        send(zsq, zsqr.at[d - 1], sz_sem.at[d - 1], at_z(d) * NX + x, t)
    for k in FAR_FIRST + (0,):
        total = yq[x, at_z(k)].astype(F32)
        for d in (1, 3, 2):
            arrived(yqr.at[d - 1, k], yq_sem.at[k * 3 + d - 1])
            total = total + yqr[d - 1, k].astype(F32)
        if k:
            zq[k - 1] = total.astype(BF16)
            send(zq.at[k - 1], zqr.at[k - 1], zq_sem.at[k - 1], at_z(k) * NX + x, t)
        else:
            queries = total

    for copy in c_route:
        copy.wait()
    names = [route[0:1], route[1:2]]
    expert = iota((32, SEQS), 0)
    chosen = (jnp.where(names[0] == expert, 1.0, 0.0) + jnp.where(names[1] == expert, 1.0, 0.0)).astype(BF16)
    before = jnp.where(iota((SEQS, SEQS), 0) < iota((SEQS, SEQS), 1), 1.0, 0.0).astype(BF16)
    earlier = jnp.dot(chosen, before, preferred_element_type=F32)
    slots = [
        n * CAP + jnp.sum(jnp.where(n == expert, earlier, 0.0), axis=0, keepdims=True).astype(jnp.int32) for n in names
    ]
    weight_sum = rweights[0:1] + rweights[1:2]
    shares = [rweights[0:1] / weight_sum, rweights[1:2] / weight_sum]
    for i in range(2):
        row = iota((128, SEQS), 0) + i * 128
        slot = lax.shift_right_logical(row, 5) * (NX * CAP) + (x * CAP + c * HALF) + (row & 31)
        pmat[i * 128 : (i + 1) * 128] = jnp.where((slots[0] == slot) | (slots[1] == slot), 1.0, 0.0).astype(BF16)
    for i in range(8):
        row = iota((128, SEQS), 0) + i * 128
        slot = lax.shift_right_logical(row, 5) * CAP + c * HALF + (row & 31)
        ctm[i * 128 : (i + 1) * 128] = jnp.where(
            slots[0] == slot, shares[0], jnp.where(slots[1] == slot, shares[1], 0.0)
        ).astype(BF16)

    sq = zsq[...]
    for d in NEAR_FIRST:
        arrived(zqr.at[d - 1], zq_sem.at[d - 1])
        arrived(zsqr.at[d - 1], sz_sem.at[d - 1])
        queries = queries + zqr[d - 1].astype(F32)
        sq = sq + zsqr[d - 1]
    lane = iota((ROWS, HD), 1)
    pick = lane == z * ROWS + iota((ROWS, HD), 0)
    mean = jnp.sum(jnp.where(pick, jnp.broadcast_to(sq[0:1], (ROWS, HD)), 0.0), axis=1, keepdims=True) / MODEL
    token_scale = lax.rsqrt(mean + EPSILON)
    queries = queries * token_scale

    q = jnp.concatenate([queries[:, 0:128], queries[:, 128:256]], axis=0).astype(BF16).astype(F32)
    seq = lax.rem(iota((2 * ROWS, 1), 0), ROWS)
    c_k.wait()
    scores = jnp.zeros((2 * ROWS, LEN), F32)
    for p in range(ROWS // 2):
        keys = jnp.concatenate([kbuf[2 * p], kbuf[2 * p + 1]], axis=1)
        own = jnp.concatenate([jnp.where(seq == 2 * p, q, 0.0), jnp.where(seq == 2 * p + 1, q, 0.0)], axis=1)
        scores = scores + lax.dot_general(own.astype(BF16), keys, (((1,), (1,)), ((), ())), preferred_element_type=F32)
    first = iota((2 * ROWS, 1), 0) < ROWS
    for copy in c_small:
        copy.wait()
    length = jnp.zeros((2 * ROWS, 1), jnp.int32)
    for s in range(ROWS):
        length = jnp.where(seq == s, lens[s], length)
    scores = scores * HD ** (-0.5) + jnp.where(first, boff[0], boff[1])
    inside = iota((2 * ROWS, LEN), 1) < length
    tail = jnp.log1p(jnp.exp(-jnp.abs(scores)))
    failed = jnp.where(inside, -(jnp.maximum(scores, 0.0) + tail), 0.0)
    blocks = [failed[:, b * 128 : (b + 1) * 128] for b in range(LEN // 128)]
    later = (iota((128, 128), 0) > iota((128, 128), 1)).astype(F32)
    within = jnp.dot(jnp.concatenate(blocks, axis=0), later, precision=HIGH, preferred_element_type=F32)
    after = jnp.zeros((2 * ROWS, 1), F32)
    sums = []
    for b in reversed(range(LEN // 128)):
        sums.insert(0, within[b * 32 : (b + 1) * 32] + after)
        after = after + jnp.sum(blocks[b], axis=1, keepdims=True)
    later_sum = jnp.concatenate(sums, axis=1)
    weights = jnp.where(inside, jnp.exp(jnp.minimum(scores, 0.0) - tail + later_sum), 0.0).astype(BF16)
    c_v.wait()
    attended = jnp.zeros((2 * ROWS, HD), F32)
    for p in range(ROWS // 2):
        vals = jnp.concatenate([vbuf[2 * p], vbuf[2 * p + 1]], axis=1)
        both = jnp.dot(weights, vals, preferred_element_type=F32)
        attended = jnp.where(seq == 2 * p, both[:, 0:128], jnp.where(seq == 2 * p + 1, both[:, 128:256], attended))
    norm = lax.rsqrt(jnp.mean(attended * attended, axis=1, keepdims=True) + EPSILON)
    head = attended * norm * jnp.where(first, hgain[0:1], hgain[1:2])
    hall[z] = jnp.concatenate([head[:ROWS], head[ROWS:]], axis=1).astype(BF16)

    for d in FAR_FIRST:
        send(hall.at[z], hall.at[z], h_sem.at[d - 1], at_z(d) * NX + x, t)
    kv = yk[x].astype(F32)
    for d in (1, 3, 2):
        arrived(ykr.at[d - 1], yk_sem.at[d - 1])
        kv = kv + ykr[d - 1].astype(F32)
    zk[...] = kv.astype(BF16)
    for d in FAR_FIRST:
        send(zk.at[at_z(d)], zkr.at[d - 1], zk_sem.at[d - 1], at_z(d) * NX + x, t)
    for d in (1, 2, 3):
        arrived(wog.at[at_x(NX - d)], wo_sem.at[d - 1])
        arrived(sres.at[at_x(NX - d)], sr_sem.at[d - 1])
        arrived(fgall.at[at_x(NX - d)], fg_sem.at[d - 1])
        arrived(wgu.at[at_x(NX - d), :, 0:128], wg_sem.at[d - 1])
        arrived(wgu.at[at_x(NX - d), :, 128:256], wu_sem.at[d - 1])
    c_dg.wait()
    c_du.wait()
    for d in NEAR_FIRST:
        arrived(hall.at[at_z(NZ - d)], h_sem.at[d - 1])
    heads = hall[...].reshape(NZ * ROWS, 256)
    for xi in range(NX):
        part = jnp.dot(heads, wog[xi], preferred_element_type=F32)
        obuf[:, :, xi * 128 : (xi + 1) * 128] = part.astype(BF16).reshape(NZ, ROWS, 128)
    for d in (4, 5, 3, 2, 6, 7, 1):
        send(obuf.at[at_t(d)], orecv.at[d - 1], o_sem.at[d - 1], e, at_t(d))
    attn = obuf[t].astype(F32)
    for d in NEAR_FIRST:
        arrived(orecv.at[d - 1], o_sem.at[d - 1])
        attn = attn + orecv[d - 1].astype(F32)
    attn = attn.astype(BF16)
    rbuf[...] = (attn.astype(F32) + jnp.concatenate([sres[xi].astype(F32) for xi in range(NX)], axis=1)).astype(BF16)

    def at_y(d):
        return lax.rem(t + 2 * d, NT)

    for dy in (2, 1, 3, 0):
        for dx in (2, 1, 3, 0):
            if dy or dx:
                send(rbuf, rall.at[t, x], r_sem.at[dy * NX + dx], z * NX + at_x(dx), at_y(dy))
    send(rbuf, rall.at[t, x], rf_sem.at[0], e, partner)
    rall[t, x] = rbuf[...]
    kv = zk[z].astype(F32)
    for d in NEAR_FIRST:
        arrived(zkr.at[d - 1], zk_sem.at[d - 1])
        kv = kv + zkr[d - 1].astype(F32)
    kv = kv * token_scale
    key_rows[...] = kv[:, 0:128].astype(BF16)
    value_rows[...] = kv[:, 128:256].astype(BF16)
    for dy in (0, 1, 3, 2):
        for dx in (0, 1, 3, 2):
            if dy or dx:
                block = rall.at[at_y(4 - dy), at_x(NX - dx)]
                arrived(block, r_sem.at[dy * NX + dx])
                send(block, block, rf_sem.at[dy * NX + dx], e, partner)
    other = lax.div(t, 2) * 2 + 1 - c
    for dy in range(4):
        for dx in range(NX):
            arrived(rall.at[lax.rem(other + 2 * (4 - dy), NT), at_x(NX - dx)], rf_sem.at[dy * NX + dx])
    gains = jnp.concatenate([fgall[xi][0:1] for xi in range(NX)], axis=1)
    square_rows = []
    for i in range(4):
        rows = rall[2 * i : 2 * i + 2].reshape(128, 512).astype(F32)
        gbuf[i * 128 : (i + 1) * 128] = (rows * gains).astype(BF16)
        squares = rows * rows
        squares = squares[:, 0:128] + squares[:, 128:256] + squares[:, 256:384] + squares[:, 384:512]
        square_rows.append(jnp.sum(squares.T, axis=0, keepdims=True))
    fsq[...] = jnp.concatenate(square_rows + [jnp.zeros((4, 128), F32)], axis=0)
    dispatched = jnp.dot(pmat[...], gbuf[...], preferred_element_type=F32)
    dbuf[...] = dispatched.astype(BF16).reshape(NZ, HALF, 512)
    for d in FAR_FIRST:
        to = at_z(d) * NX + x
        send(dbuf.at[at_z(d)], xe.at[c, z], d_sem.at[d - 1], to, t)
        send(fsq, fsqr.at[d - 1], fs_sem.at[d - 1], to, t)
    xe[c, z] = dbuf[z]
    wide = wgu[...].reshape(512, 256)
    for i in range(4):
        part = jnp.dot(gbuf[i * 128 : (i + 1) * 128], wide, preferred_element_type=F32)
        gub[2 * i : 2 * i + 2] = part.astype(BF16).reshape(2, 64, 256)
    for d in FAR_FIRST:
        send(gub.at[at_z(d)], gurecv.at[d - 1], gu_sem.at[d - 1], at_z(d) * NX + x, t)

    send(xe.at[c, z], xe.at[c, z], xe_sem.at[0], e, partner)
    for d in NEAR_FIRST:
        arrived(xe.at[c, at_z(NZ - d)], d_sem.at[d - 1])
        send(xe.at[c, at_z(NZ - d)], xe.at[c, at_z(NZ - d)], xe_sem.at[d], e, partner)
    sq = fsq[...]
    for d in NEAR_FIRST:
        arrived(fsqr.at[d - 1], fs_sem.at[d - 1])
        sq = sq + fsqr[d - 1]
    inverse = lax.rsqrt(sq / MODEL + EPSILON)
    inverse = jnp.concatenate([inverse[i : i + 1] for i in range(4)], axis=1)
    slot = iota((CAP, SEQS), 0) + e * CAP
    mine = (slots[0] == slot) | (slots[1] == slot)
    slot_scale = jnp.sum(jnp.where(mine, jnp.broadcast_to(inverse, (CAP, SEQS)), 0.0), axis=1, keepdims=True)
    own_row = iota((64, SEQS), 1) == iota((64, SEQS), 0) + z * 64
    row_scale = jnp.sum(jnp.where(own_row, jnp.broadcast_to(inverse, (64, SEQS)), 0.0), axis=1, keepdims=True)
    c_eg.wait()
    c_eu.wait()
    acc = jnp.zeros((CAP, 256), F32)
    for d in (0,) + NEAR_FIRST:
        zs = at_z(NZ - d)
        arrived(xe.at[1 - c, zs], xe_sem.at[d])
        rows = jnp.concatenate([xe[0, zs], xe[1, zs]], axis=0)
        both = jnp.concatenate([egb[zs], eub[zs]], axis=1)
        acc = acc + jnp.dot(rows, both, preferred_element_type=F32)
    acc = acc * slot_scale
    gate = acc[:, 0:128]
    hidden = (gate / (1.0 + jnp.exp(-gate)) * acc[:, 128:256]).astype(BF16)
    for copy in c_ed:
        copy.wait()
    for k, d in enumerate(FAR_FIRST + (0,)):
        zi = at_z(d)
        part = jnp.dot(hidden, edb[zi], preferred_element_type=F32)
        kept = jnp.where(c == 0, part[:HALF], part[HALF:]).astype(BF16)
        given = jnp.where(c == 0, part[HALF:], part[:HALF]).astype(BF16)
        for xi in range(NX):
            pown[zi, xi] = kept[:, xi * 128 : (xi + 1) * 128]
            pout[zi, xi] = given[:, xi * 128 : (xi + 1) * 128]
        send(pout.at[zi], precv.at[zi], p_sem.at[k], e, partner)

    gu = gub[z].astype(F32)
    for d in NEAR_FIRST:
        arrived(gurecv.at[d - 1], gu_sem.at[d - 1])
        gu = gu + gurecv[d - 1].astype(F32)
    gu = gu * row_scale
    gate = gu[:, 0:128]
    hd[x, z] = (gate / (1.0 + jnp.exp(-gate)) * gu[:, 128:256]).astype(BF16)
    for d in FAR_FIRST:
        send(hd.at[x, z], hd.at[x, z], hz_sem.at[d - 1], at_z(d) * NX + x, t)

    for k, d in enumerate(FAR_FIRST + (0,)):
        zi = at_z(d)
        arrived(precv.at[zi], p_sem.at[k])
        rsum[zi] = (pown[zi].astype(F32) + precv[zi].astype(F32)).astype(BF16)
        for dx in (2, 1, 3, 0):
            if d or dx:
                send(rsum.at[zi, at_x(dx)], rt.at[e], rt_sem.at[d * NX + dx], zi * NX + at_x(dx), t)
    rt[e] = rsum[z, x]

    for dx in (2, 1, 3):
        send(hd.at[x, z], hd.at[x, z], hx_sem.at[dx - 1], z * NX + at_x(dx), t)
    for d in NEAR_FIRST:
        zs = at_z(NZ - d)
        arrived(hd.at[x, zs], hz_sem.at[d - 1])
        for dx in (2, 1, 3):
            send(hd.at[x, zs], hd.at[x, zs], hx_sem.at[d * 3 + dx - 1], z * NX + at_x(dx), t)

    for d in range(NZ):
        for dx in range(NX):
            if d or dx:
                arrived(rt.at[at_z(NZ - d) * NX + at_x(NX - dx)], rt_sem.at[d * NX + dx])
    moe = lax.dot_general(ctm[...], rt[...].reshape(1024, 128), (((0,), (0,)), ((), ())), preferred_element_type=F32)
    for d in (0,) + NEAR_FIRST:
        for dx in (1, 3, 2):
            arrived(hd.at[at_x(NX - dx), at_z(NZ - d)], hx_sem.at[d * 3 + dx - 1])
    c_dd.wait()
    dense = jnp.zeros((SEQS, 128), F32)
    for xi in range(NX):
        dense = dense + jnp.dot(hd[xi].reshape(SEQS, 128), ddb[xi * 128 : (xi + 1) * 128], preferred_element_type=F32)
    fbuf[...] = (moe + mgain[...] * dense).astype(BF16).reshape(2, 256, 128)

    send(fbuf.at[1 - c], fpair, f_sem.at[0], e, partner)
    out = fbuf[c].astype(F32)
    arrived(fpair, f_sem.at[0])
    out = out + fpair[...].astype(F32)
    fhalf[...] = out.astype(BF16)
    for d in (2, 1, 3):
        send(fhalf, frecv.at[d - 1], f_sem.at[d], e, at_y(d))
    mine = pl.ds(pl.multiple_of(x * 128, 128), 128)
    out = out + rall[pl.ds(c * 4, 4), :, :, mine].reshape(256, 128).astype(F32)
    for d in (1, 3, 2):
        arrived(frecv.at[d - 1], f_sem.at[d])
        out = out + frecv[d - 1].astype(F32)
    mgath[c] = out.astype(BF16)
    send(mgath.at[c], mgath.at[c], m_sem.at[0], e, partner)
    arrived(mgath.at[1 - c], m_sem.at[0])
    mixed[...] = mgath[...].reshape(SEQS, 128)
    for copy in started:
        copy.wait_send()


def finish_kernel(a, b, c, a_out, b_out, c_out):
    a_out[...] = a[...]
    b_out[...] = b[...]
    c_out[...] = c[...]


def per_device(
    stream, norm_gain, w_query, w_key, w_value, break_offset, cache_keys, cache_values, lengths, w_output, head_gain,
    ffn_gain, route_experts, route_weights, expert_gate, expert_up, expert_down, dense_gate, dense_up, dense_down, mix_gain,
):
    any_spec = pl.BlockSpec(memory_space=pl.ANY)
    vm = pl.BlockSpec(memory_space=pltpu.VMEM)
    dma = pltpu.SemaphoreType.DMA

    def b(*shape):
        return pltpu.VMEM(shape, BF16)

    def f(*shape):
        return pltpu.VMEM(shape, F32)

    scratch = dict(
        ngain=f(1, 128), hgain=f(2, 128), fgain=f(1, 128), mgain=f(1, 128),
        route=pltpu.VMEM((2, SEQS), jnp.int32), rweights=f(2, SEQS), boff=pltpu.SMEM((2,), F32), lens=pltpu.SMEM((ROWS,), jnp.int32),
        strm=b(NX, NZ, ROWS, 128), wqkv=b(128, 512), kbuf=b(ROWS, LEN, 128), vbuf=b(ROWS, LEN, 128),
        xgain=b(NX, 128, 128), yq=b(NX, NZ, ROWS, 256), yqr=b(NX - 1, NZ, ROWS, 256),
        yk=b(NX, NZ, ROWS, 256), ykr=b(NX - 1, NZ, ROWS, 256), ssq=f(NX, 8, 128), ssqr=f(NX - 1, 8, 128),
        zq=b(NZ - 1, ROWS, 256), zqr=b(NZ - 1, ROWS, 256), zk=b(NZ, ROWS, 256), zkr=b(NZ - 1, ROWS, 256),
        zsq=f(8, 128), zsqr=f(NZ - 1, 8, 128),
        wog=b(NX, 256, 128), hall=b(NZ, ROWS, 256), obuf=b(NZ, ROWS, 512), orecv=b(NT - 1, ROWS, 512),
        sres=b(NX, ROWS, 128), fgb=f(8, 128), fgall=f(NX, 8, 128),
        wgu=b(NX, 128, 256), ddb=b(512, 128), egb=b(NZ, 512, 128), eub=b(NZ, 512, 128), edb=b(NZ, 128, 512),
        pmat=b(256, SEQS), ctm=b(1024, SEQS), rbuf=b(ROWS, 512), rall=b(NT, NX, ROWS, 512), gbuf=b(SEQS, 512),
        fsq=f(8, 128), fsqr=f(NZ - 1, 8, 128), gub=b(NZ, 64, 256), gurecv=b(NZ - 1, 64, 256),
        dbuf=b(NZ, HALF, 512), xe=b(2, NZ, HALF, 512), hd=b(NX, NZ, 64, 128),
        pown=b(NZ, NX, HALF, 128), pout=b(NZ, NX, HALF, 128), precv=b(NZ, NX, HALF, 128), rsum=b(NZ, NX, HALF, 128),
        rt=b(32, HALF, 128), fbuf=b(2, 256, 128), fpair=b(256, 128), fhalf=b(256, 128), frecv=b(3, 256, 128), mgath=b(2, 256, 128),
        lsem=dma((32,)), ssem=dma((224,)), ring_sem=pltpu.SemaphoreType.REGULAR((4,)),
        yq_sem=dma((24,)), yk_sem=dma((3,)), sx_sem=dma((3,)), wo_sem=dma((3,)), wg_sem=dma((3,)), wu_sem=dma((3,)),
        sr_sem=dma((3,)), fg_sem=dma((3,)), zq_sem=dma((7,)), zk_sem=dma((7,)), sz_sem=dma((7,)), h_sem=dma((7,)), o_sem=dma((7,)),
        r_sem=dma((16,)), rf_sem=dma((16,)),
        fs_sem=dma((7,)), gu_sem=dma((7,)), d_sem=dma((7,)), xe_sem=dma((8,)), hz_sem=dma((7,)),
        hx_sem=dma((24,)), p_sem=dma((8,)), rt_sem=dma((32,)), f_sem=dma((4,)), m_sem=dma((1,)),
    )
    results = pl.pallas_call(
        step_kernel,
        name="step",
        out_shape=(
            jax.ShapeDtypeStruct((SEQS, 128), BF16),
            jax.ShapeDtypeStruct((ROWS, 128), BF16),
            jax.ShapeDtypeStruct((ROWS, 128), BF16),
        ),
        in_specs=[any_spec] * 21,
        out_specs=(vm, vm, vm),
        scratch_shapes=list(scratch.values()),
        compiler_params=pltpu.CompilerParams(collective_id=0, has_side_effects=True, vmem_limit_bytes=60 * 1024 * 1024),
    )(
        stream.reshape(NZ, NX, ROWS, 128), w_query, w_key, w_value,
        cache_keys.reshape(ROWS, LEN, 128), cache_values.reshape(ROWS, LEN, 128), w_output,
        expert_gate.reshape(NZ, 512, 128), expert_up.reshape(NZ, 512, 128), expert_down.reshape(128, MODEL),
        dense_gate, dense_up, dense_down,
        norm_gain.reshape(1, 128), head_gain.reshape(2, 128), ffn_gain.reshape(1, 128), mix_gain.reshape(1, 128),
        route_experts.T, route_weights.T, break_offset, lengths,
    )
    return pl.pallas_call(
        finish_kernel,
        name="finish",
        out_shape=tuple(jax.ShapeDtypeStruct(r.shape, r.dtype) for r in results),
        in_specs=[vm] * 3,
        out_specs=(vm,) * 3,
    )(*results)


def solution(mesh):
    in_specs = (
        P(None, "ep"),
        P("ep"),
        P("ep", "tp"),
        P("ep", "tp"),
        P("ep", "tp"),
        P("tp"),
        P("ep", None, "tp", None),
        P("ep", None, "tp", None),
        P("ep"),
        P("tp", "ep"),
        P("tp"),
        P("ep"),
        P(),
        P(),
        P("ep", None, "tp"),
        P("ep", None, "tp"),
        P("ep", "tp", None),
        P("ep", "tp"),
        P("ep", "tp"),
        P("tp", "ep"),
        P("ep"),
    )
    out_specs = (P(None, "ep"), P("ep", "tp"), P("ep", "tp"))
    return jax.shard_map(
        per_device, mesh=mesh, in_specs=in_specs, out_specs=out_specs, check_vma=False
    )
```

```python
import jax
import jax.numpy as jnp
from jax import lax
from jax.experimental import pallas as pl
from jax.experimental.pallas import tpu as pltpu
from jax.sharding import PartitionSpec as P

EPSILON = 1e-06
NX, NZ, NT = 4, 8, 8
MODEL, HD, LEN, ROWS, SEQS = 4096, 128, 1024, 16, 512
CAP, HALF = 64, 32
F32, BF16 = jnp.float32, jnp.bfloat16
HIGH = lax.Precision.HIGHEST
MESH = pl.DeviceIdType.MESH
FAR_FIRST = (4, 3, 5, 2, 6, 1, 7)
NEAR_FIRST = (1, 7, 2, 6, 3, 5, 4)


def iota(shape, dim):
    return lax.broadcasted_iota(jnp.int32, shape, dim)


def step_kernel(
    stream, wq, wk, wv, ck, cv, wo, eg, eu, ed, dg, du, dd,
    ngain_hbm, hgain_hbm, fgain_hbm, mgain_hbm, route_hbm, rweights_hbm, boff_hbm, lens_hbm,
    mixed, key_rows, value_rows,
    ngain, hgain, fgain, mgain, route, rweights, boff, lens,
    strm, wqkv, kbuf, vbuf, xgain, yq, yqr, yk, ykr, ssq, ssqr, zq, zqr, zk, zkr, zsq, zsqr,
    wog, hall, obuf, orecv, sres, fgb, fgall, wgu, ddb, egb, eub, edb,
    pmat, ctm, rbuf, rall, gbuf, fsq, fsqr, gub, gurecv, dbuf, xe, hd,
    pown, pout, precv, rsum, ysum, back, rt, fbuf, fpair, fhalf, frecv, mgath,
    lsem, ssem, ring_sem,
    yq_sem, yk_sem, sx_sem, wo_sem, wg_sem, wu_sem, sr_sem, fg_sem, zq_sem, zk_sem, sz_sem, h_sem, o_sem, r_sem, rf_sem,
    fs_sem, gu_sem, d_sem, xy_sem, xe_sem, hz_sem, hx_sem, p_sem, ys_sem, rt_sem, f_sem, m_sem,
):
    e = lax.axis_index("ep")
    t = lax.axis_index("tp")
    z = lax.div(e, NX)
    x = lax.rem(e, NX)
    c = lax.rem(t, 2)
    partner = t + 1 - 2 * c

    def at_x(d):
        return lax.rem(x + d, NX)

    def at_z(d):
        return lax.rem(z + d, NZ)

    def at_t(d):
        return lax.rem(t + d, NT)

    started = []

    def send(src, dst, rsem, dev_e, dev_t):
        copy = pltpu.make_async_remote_copy(
            src_ref=src, dst_ref=dst, send_sem=ssem.at[len(started)], recv_sem=rsem,
            device_id=(dev_e, dev_t), device_id_type=MESH,
        )
        copy.start()
        started.append(copy)

    def arrived(dst, rsem):
        pltpu.make_async_copy(dst, dst, rsem).wait()

    loads = []

    def load(src, dst):
        copy = pltpu.make_async_copy(src, dst, lsem.at[len(loads)])
        copy.start()
        loads.append(copy)
        return copy

    def columns(ref, block):
        return ref.at[:, pl.ds(pl.multiple_of(block * 128, 128), 128)]

    def signal(sem, dev_e, dev_t):
        pl.semaphore_signal(sem, inc=1, device_id=(dev_e, dev_t), device_id_type=MESH)

    barrier = pltpu.get_barrier_semaphore()
    for d in (1, NZ - 1):
        signal(barrier, at_z(d) * NX + x, t)
    for d in range(1, NX):
        signal(barrier, z * NX + at_x(d), t)
    for d in range(1, NT):
        signal(barrier, e, at_t(d))

    c_s = [load(stream.at[:, xi], strm.at[xi]) for xi in range(NX)]
    c_w = [load(ngain_hbm, ngain), load(wq, wqkv.at[:, 0:256]), load(wk, wqkv.at[:, 256:384]), load(wv, wqkv.at[:, 384:512])]
    c_route = [load(route_hbm, route), load(rweights_hbm, rweights)]
    c_small = [load(hgain_hbm, hgain), load(mgain_hbm, mgain), load(boff_hbm, boff), load(lens_hbm, lens)]
    c_fg = load(fgain_hbm, fgain)
    c_wo = load(wo, wog.at[x])
    c_k = load(ck, kbuf)
    c_v = load(cv, vbuf)
    c_dg = load(columns(dg, x), wgu.at[x, :, 0:128])
    c_du = load(columns(du, x), wgu.at[x, :, 128:256])
    c_dd = load(dd, ddb)
    c_eg = load(eg, egb)
    c_eu = load(eu, eub)
    c_ed = [load(ed.at[:, zi * 512 : (zi + 1) * 512], edb.at[zi]) for zi in range(NZ)]

    for copy in c_s + c_w:
        copy.wait()
    gain = ngain[...]
    w = wqkv[...]
    for xi in range(NX):
        rows = strm[xi].reshape(NZ * ROWS, HD).astype(F32)
        scaled = (rows * gain).astype(BF16)
        xgain[xi] = scaled
        yq[xi] = jnp.dot(scaled, w[:, 0:256], preferred_element_type=F32).astype(BF16).reshape(NZ, ROWS, 256)
        sums = jnp.sum((rows * rows).T, axis=0, keepdims=True)
        ssq[xi] = jnp.broadcast_to(sums, (8, HD))
    c_fg.wait()
    fgb[...] = jnp.broadcast_to(fgain[...], (8, HD))

    pl.semaphore_wait(barrier, 2 + NX - 1 + NT - 1)

    for d in (2, 1, 3):
        send(ssq.at[at_x(d)], ssqr.at[d - 1], sx_sem.at[d - 1], z * NX + at_x(d), t)
    for k in FAR_FIRST + (0,):
        for d in (2, 1, 3):
            send(yq.at[at_x(d), at_z(k)], yqr.at[d - 1, k], yq_sem.at[k * 3 + d - 1], z * NX + at_x(d), t)
    signal(ring_sem.at[0], at_z(1) * NX + x, t)
    signal(ring_sem.at[1], at_z(7) * NX + x, t)
    c_wo.wait()
    for d in (2, 1, 3):
        to = z * NX + at_x(d)
        send(wog.at[x], wog.at[x], wo_sem.at[d - 1], to, t)
        send(strm.at[at_x(d), t], sres.at[x], sr_sem.at[d - 1], to, t)
        send(fgb, fgall.at[x], fg_sem.at[d - 1], to, t)
    sres[x] = strm[x, t]
    fgall[x] = fgb[...]
    pl.semaphore_wait(ring_sem.at[0], 1)
    pl.semaphore_wait(ring_sem.at[1], 1)
    signal(ring_sem.at[2], at_z(2) * NX + x, t)
    signal(ring_sem.at[3], at_z(6) * NX + x, t)
    for xi in range(NX):
        yk[xi] = jnp.dot(xgain[xi], w[:, 256:512], preferred_element_type=F32).astype(BF16).reshape(NZ, ROWS, 256)
    for d in (2, 1, 3):
        send(yk.at[at_x(d)], ykr.at[d - 1], yk_sem.at[d - 1], z * NX + at_x(d), t)
    for d in (2, 1, 3):
        to = z * NX + at_x(d)
        send(columns(dg, at_x(d)), wgu.at[x, :, 0:128], wg_sem.at[d - 1], to, t)
        send(columns(du, at_x(d)), wgu.at[x, :, 128:256], wu_sem.at[d - 1], to, t)
    pl.semaphore_wait(ring_sem.at[2], 1)
    pl.semaphore_wait(ring_sem.at[3], 1)

    sq = ssq[x]
    for d in (1, 3, 2):
        arrived(ssqr.at[d - 1], sx_sem.at[d - 1])
        sq = sq + ssqr[d - 1]
    zsq[...] = sq
    for d in FAR_FIRST:
        send(zsq, zsqr.at[d - 1], sz_sem.at[d - 1], at_z(d) * NX + x, t)
    for k in FAR_FIRST + (0,):
        total = yq[x, at_z(k)].astype(F32)
        for d in (1, 3, 2):
            arrived(yqr.at[d - 1, k], yq_sem.at[k * 3 + d - 1])
            total = total + yqr[d - 1, k].astype(F32)
        if k:
            zq[k - 1] = total.astype(BF16)
            send(zq.at[k - 1], zqr.at[k - 1], zq_sem.at[k - 1], at_z(k) * NX + x, t)
        else:
            queries = total

    for copy in c_route:
        copy.wait()
    names = [route[0:1], route[1:2]]
    expert = iota((32, SEQS), 0)
    chosen = (jnp.where(names[0] == expert, 1.0, 0.0) + jnp.where(names[1] == expert, 1.0, 0.0)).astype(BF16)
    before = jnp.where(iota((SEQS, SEQS), 0) < iota((SEQS, SEQS), 1), 1.0, 0.0).astype(BF16)
    earlier = jnp.dot(chosen, before, preferred_element_type=F32)
    slots = [
        n * CAP + jnp.sum(jnp.where(n == expert, earlier, 0.0), axis=0, keepdims=True).astype(jnp.int32) for n in names
    ]
    weight_sum = rweights[0:1] + rweights[1:2]
    shares = [rweights[0:1] / weight_sum, rweights[1:2] / weight_sum]
    y = lax.div(t, 2)
    row = iota((64, SEQS), 0)
    slot = lax.shift_right_logical(row, 3) * (NX * CAP) + (x * CAP + c * HALF + y * 8) + (row & 7)
    pmat[...] = jnp.where((slots[0] == slot) | (slots[1] == slot), 1.0, 0.0).astype(BF16)
    for i in range(2):
        row = iota((128, SEQS), 0) + i * 128
        slot = lax.shift_right_logical(row, 3) * CAP + c * HALF + y * 8 + (row & 7)
        ctm[i * 128 : (i + 1) * 128] = jnp.where(
            slots[0] == slot, shares[0], jnp.where(slots[1] == slot, shares[1], 0.0)
        ).astype(BF16)

    sq = zsq[...]
    for d in NEAR_FIRST:
        arrived(zqr.at[d - 1], zq_sem.at[d - 1])
        arrived(zsqr.at[d - 1], sz_sem.at[d - 1])
        queries = queries + zqr[d - 1].astype(F32)
        sq = sq + zsqr[d - 1]
    lane = iota((ROWS, HD), 1)
    pick = lane == z * ROWS + iota((ROWS, HD), 0)
    mean = jnp.sum(jnp.where(pick, jnp.broadcast_to(sq[0:1], (ROWS, HD)), 0.0), axis=1, keepdims=True) / MODEL
    token_scale = lax.rsqrt(mean + EPSILON)
    queries = queries * token_scale

    q = jnp.concatenate([queries[:, 0:128], queries[:, 128:256]], axis=0).astype(BF16).astype(F32)
    seq = lax.rem(iota((2 * ROWS, 1), 0), ROWS)
    c_k.wait()
    scores = jnp.zeros((2 * ROWS, LEN), F32)
    for p in range(ROWS // 2):
        keys = jnp.concatenate([kbuf[2 * p], kbuf[2 * p + 1]], axis=1)
        own = jnp.concatenate([jnp.where(seq == 2 * p, q, 0.0), jnp.where(seq == 2 * p + 1, q, 0.0)], axis=1)
        scores = scores + lax.dot_general(own.astype(BF16), keys, (((1,), (1,)), ((), ())), preferred_element_type=F32)
    first = iota((2 * ROWS, 1), 0) < ROWS
    for copy in c_small:
        copy.wait()
    length = jnp.zeros((2 * ROWS, 1), jnp.int32)
    for s in range(ROWS):
        length = jnp.where(seq == s, lens[s], length)
    scores = scores * HD ** (-0.5) + jnp.where(first, boff[0], boff[1])
    inside = iota((2 * ROWS, LEN), 1) < length
    tail = jnp.log1p(jnp.exp(-jnp.abs(scores)))
    failed = jnp.where(inside, -(jnp.maximum(scores, 0.0) + tail), 0.0)
    blocks = [failed[:, b * 128 : (b + 1) * 128] for b in range(LEN // 128)]
    later = (iota((128, 128), 0) > iota((128, 128), 1)).astype(F32)
    within = jnp.dot(jnp.concatenate(blocks, axis=0), later, precision=HIGH, preferred_element_type=F32)
    after = jnp.zeros((2 * ROWS, 1), F32)
    sums = []
    for b in reversed(range(LEN // 128)):
        sums.insert(0, within[b * 32 : (b + 1) * 32] + after)
        after = after + jnp.sum(blocks[b], axis=1, keepdims=True)
    later_sum = jnp.concatenate(sums, axis=1)
    weights = jnp.where(inside, jnp.exp(jnp.minimum(scores, 0.0) - tail + later_sum), 0.0).astype(BF16)
    c_v.wait()
    attended = jnp.zeros((2 * ROWS, HD), F32)
    for p in range(ROWS // 2):
        vals = jnp.concatenate([vbuf[2 * p], vbuf[2 * p + 1]], axis=1)
        both = jnp.dot(weights, vals, preferred_element_type=F32)
        attended = jnp.where(seq == 2 * p, both[:, 0:128], jnp.where(seq == 2 * p + 1, both[:, 128:256], attended))
    norm = lax.rsqrt(jnp.mean(attended * attended, axis=1, keepdims=True) + EPSILON)
    head = attended * norm * jnp.where(first, hgain[0:1], hgain[1:2])
    hall[z] = jnp.concatenate([head[:ROWS], head[ROWS:]], axis=1).astype(BF16)

    for d in FAR_FIRST:
        send(hall.at[z], hall.at[z], h_sem.at[d - 1], at_z(d) * NX + x, t)
    kv = yk[x].astype(F32)
    for d in (1, 3, 2):
        arrived(ykr.at[d - 1], yk_sem.at[d - 1])
        kv = kv + ykr[d - 1].astype(F32)
    zk[...] = kv.astype(BF16)
    for d in FAR_FIRST:
        send(zk.at[at_z(d)], zkr.at[d - 1], zk_sem.at[d - 1], at_z(d) * NX + x, t)
    for d in (1, 2, 3):
        arrived(wog.at[at_x(NX - d)], wo_sem.at[d - 1])
        arrived(sres.at[at_x(NX - d)], sr_sem.at[d - 1])
        arrived(fgall.at[at_x(NX - d)], fg_sem.at[d - 1])
        arrived(wgu.at[at_x(NX - d), :, 0:128], wg_sem.at[d - 1])
        arrived(wgu.at[at_x(NX - d), :, 128:256], wu_sem.at[d - 1])
    c_dg.wait()
    c_du.wait()
    for d in NEAR_FIRST:
        arrived(hall.at[at_z(NZ - d)], h_sem.at[d - 1])
    heads = hall[...].reshape(NZ * ROWS, 256)
    for xi in range(NX):
        part = jnp.dot(heads, wog[xi], preferred_element_type=F32)
        obuf[:, :, xi * 128 : (xi + 1) * 128] = part.astype(BF16).reshape(NZ, ROWS, 128)
    for d in (4, 5, 3, 2, 6, 7, 1):
        send(obuf.at[at_t(d)], orecv.at[d - 1], o_sem.at[d - 1], e, at_t(d))
    attn = obuf[t].astype(F32)
    for d in NEAR_FIRST:
        arrived(orecv.at[d - 1], o_sem.at[d - 1])
        attn = attn + orecv[d - 1].astype(F32)
    attn = attn.astype(BF16)
    rbuf[...] = (attn.astype(F32) + jnp.concatenate([sres[xi].astype(F32) for xi in range(NX)], axis=1)).astype(BF16)

    def at_y(d):
        return lax.rem(t + 2 * d, NT)

    for dy in (2, 1, 3, 0):
        for dx in (2, 1, 3, 0):
            if dy or dx:
                send(rbuf, rall.at[t, x], r_sem.at[dy * NX + dx], z * NX + at_x(dx), at_y(dy))
    send(rbuf, rall.at[t, x], rf_sem.at[0], e, partner)
    rall[t, x] = rbuf[...]
    kv = zk[z].astype(F32)
    for d in NEAR_FIRST:
        arrived(zkr.at[d - 1], zk_sem.at[d - 1])
        kv = kv + zkr[d - 1].astype(F32)
    kv = kv * token_scale
    key_rows[...] = kv[:, 0:128].astype(BF16)
    value_rows[...] = kv[:, 128:256].astype(BF16)
    for dy in (0, 1, 3, 2):
        for dx in (0, 1, 3, 2):
            if dy or dx:
                block = rall.at[at_y(4 - dy), at_x(NX - dx)]
                arrived(block, r_sem.at[dy * NX + dx])
                send(block, block, rf_sem.at[dy * NX + dx], e, partner)
    other = lax.div(t, 2) * 2 + 1 - c
    for dy in range(4):
        for dx in range(NX):
            arrived(rall.at[lax.rem(other + 2 * (4 - dy), NT), at_x(NX - dx)], rf_sem.at[dy * NX + dx])
    gains = jnp.concatenate([fgall[xi][0:1] for xi in range(NX)], axis=1)
    square_rows = []
    for i in range(4):
        rows = rall[2 * i : 2 * i + 2].reshape(128, 512).astype(F32)
        gbuf[i * 128 : (i + 1) * 128] = (rows * gains).astype(BF16)
        squares = rows * rows
        squares = squares[:, 0:128] + squares[:, 128:256] + squares[:, 256:384] + squares[:, 384:512]
        square_rows.append(jnp.sum(squares.T, axis=0, keepdims=True))
    fsq[...] = jnp.concatenate(square_rows + [jnp.zeros((4, 128), F32)], axis=0)
    dispatched = jnp.dot(pmat[...], gbuf[...], preferred_element_type=F32)
    dbuf[...] = dispatched.reshape(NZ, 8, 512).astype(BF16)
    for d in FAR_FIRST:
        to = at_z(d) * NX + x
        send(dbuf.at[at_z(d)], xe.at[t, z], d_sem.at[d - 1], to, t)
        send(fsq, fsqr.at[d - 1], fs_sem.at[d - 1], to, t)
    xe[t, z] = dbuf[z]
    wide = wgu[...].reshape(512, 256)
    for i in range(4):
        part = jnp.dot(gbuf[i * 128 : (i + 1) * 128], wide, preferred_element_type=F32)
        gub[2 * i : 2 * i + 2] = part.astype(BF16).reshape(2, 64, 256)
    for d in FAR_FIRST:
        send(gub.at[at_z(d)], gurecv.at[d - 1], gu_sem.at[d - 1], at_z(d) * NX + x, t)

    def spread(d):
        block = xe.at[t, at_z(NZ - d)]
        if d:
            arrived(block, d_sem.at[d - 1])
        for dy in (2, 1, 3):
            send(block, block, xy_sem.at[d * 3 + dy - 1], e, at_y(dy))
        send(block, block, xe_sem.at[d * 4], e, partner)

    for d in (0,) + NEAR_FIRST:
        spread(d)
    sq = fsq[...]
    for d in NEAR_FIRST:
        arrived(fsqr.at[d - 1], fs_sem.at[d - 1])
        sq = sq + fsqr[d - 1]
    inverse = lax.rsqrt(sq / MODEL + EPSILON)
    inverse = jnp.concatenate([inverse[i : i + 1] for i in range(4)], axis=1)
    slot = iota((CAP, SEQS), 0) + e * CAP
    mine = (slots[0] == slot) | (slots[1] == slot)
    slot_scale = jnp.sum(jnp.where(mine, jnp.broadcast_to(inverse, (CAP, SEQS)), 0.0), axis=1, keepdims=True)
    own_row = iota((64, SEQS), 1) == iota((64, SEQS), 0) + z * 64
    row_scale = jnp.sum(jnp.where(own_row, jnp.broadcast_to(inverse, (64, SEQS)), 0.0), axis=1, keepdims=True)
    c_eg.wait()
    c_eu.wait()
    def product(core, zs):
        rows = jnp.concatenate([xe[2 * yi + core, zs].astype(F32) for yi in range(4)], axis=0).astype(BF16)
        both = jnp.concatenate([egb[zs], eub[zs]], axis=1)
        return jnp.dot(rows, both, preferred_element_type=F32)

    near = jnp.zeros((HALF, 256), F32)
    for d in (0,) + NEAR_FIRST:
        zs = at_z(NZ - d)
        for dy in (1, 3, 2):
            block = xe.at[at_y(4 - dy), zs]
            arrived(block, xy_sem.at[d * 3 + dy - 1])
            send(block, block, xe_sem.at[d * 4 + dy], e, partner)
        near = near + product(c, zs)

    gu = gub[z].astype(F32)
    for d in NEAR_FIRST:
        arrived(gurecv.at[d - 1], gu_sem.at[d - 1])
        gu = gu + gurecv[d - 1].astype(F32)
    gu = gu * row_scale
    gate = gu[:, 0:128]
    hd[x, z] = (gate / (1.0 + jnp.exp(-gate)) * gu[:, 128:256]).astype(BF16)
    for d in FAR_FIRST:
        send(hd.at[x, z], hd.at[x, z], hz_sem.at[d - 1], at_z(d) * NX + x, t)

    across = jnp.zeros((HALF, 256), F32)
    for d in (0,) + NEAR_FIRST:
        zs = at_z(NZ - d)
        for dy in (0, 1, 3, 2):
            arrived(xe.at[lax.rem(partner + 2 * (4 - dy), NT), zs], xe_sem.at[d * 4 + dy])
        across = across + product(1 - c, zs)
    acc = jnp.concatenate([jnp.where(c == 0, near, across), jnp.where(c == 0, across, near)], axis=0)
    acc = acc * slot_scale
    gate = acc[:, 0:128]
    hidden = (gate / (1.0 + jnp.exp(-gate)) * acc[:, 128:256]).astype(BF16)
    for copy in c_ed:
        copy.wait()
    for k, d in enumerate(FAR_FIRST + (0,)):
        zi = at_z(d)
        part = jnp.dot(hidden, edb[zi], preferred_element_type=F32)
        kept = jnp.where(c == 0, part[:HALF], part[HALF:]).astype(BF16)
        given = jnp.where(c == 0, part[HALF:], part[:HALF]).astype(BF16)
        for xi in range(NX):
            pown[zi, xi] = kept[:, xi * 128 : (xi + 1) * 128]
            pout[zi, xi] = given[:, xi * 128 : (xi + 1) * 128]
        send(pout.at[zi], precv.at[zi], p_sem.at[k], e, partner)

    for k, d in enumerate(FAR_FIRST + (0,)):
        zi = at_z(d)
        arrived(precv.at[zi], p_sem.at[k])
        pair = pown[zi].astype(F32) + precv[zi].astype(F32)
        for yi in range(4):
            rsum[zi, yi] = jnp.concatenate([pair[xi, yi * 8 : (yi + 1) * 8] for xi in range(NX)], axis=0).astype(BF16)
        for dy in (2, 1, 3):
            send(rsum.at[zi, lax.rem(y + dy, 4)], ysum.at[dy - 1, zi], ys_sem.at[k * 3 + dy - 1], e, at_y(dy))

    def onward(d):
        block = hd.at[x, at_z(NZ - d)]
        if d:
            arrived(block, hz_sem.at[d - 1])
        for dx in (2, 1, 3):
            send(block, block, hx_sem.at[d * 3 + dx - 1], z * NX + at_x(dx), t)

    for d in (0, 1, 7, 2, 6):
        onward(d)
    for k, d in enumerate(FAR_FIRST + (0,)):
        zi = at_z(d)
        whole = rsum[zi, y].astype(F32)
        for dy in (1, 3, 2):
            arrived(ysum.at[dy - 1, zi], ys_sem.at[k * 3 + dy - 1])
            whole = whole + ysum[dy - 1, zi].astype(F32)
        for xi in range(NX):
            back[zi, xi] = whole[xi * 8 : (xi + 1) * 8].astype(BF16)
        for dx in (2, 1, 3, 0):
            if d or dx:
                send(back.at[zi, at_x(dx)], rt.at[e], rt_sem.at[d * NX + dx], zi * NX + at_x(dx), t)
    rt[e] = back[z, x]
    for d in (3, 5, 4):
        onward(d)

    for d in range(NZ):
        for dx in range(NX):
            if d or dx:
                arrived(rt.at[at_z(NZ - d) * NX + at_x(NX - dx)], rt_sem.at[d * NX + dx])
    returned = rt[...].astype(F32).reshape(256, 128).astype(BF16)
    moe = lax.dot_general(ctm[...], returned, (((0,), (0,)), ((), ())), preferred_element_type=F32)
    for d in (0,) + NEAR_FIRST:
        for dx in (1, 3, 2):
            arrived(hd.at[at_x(NX - dx), at_z(NZ - d)], hx_sem.at[d * 3 + dx - 1])
    c_dd.wait()
    dense = jnp.zeros((SEQS, 128), F32)
    for xi in range(NX):
        dense = dense + jnp.dot(hd[xi].reshape(SEQS, 128), ddb[xi * 128 : (xi + 1) * 128], preferred_element_type=F32)
    fbuf[...] = (moe + mgain[...] * dense).astype(BF16).reshape(2, 256, 128)

    send(fbuf.at[1 - c], fpair, f_sem.at[0], e, partner)
    out = fbuf[c].astype(F32)
    arrived(fpair, f_sem.at[0])
    out = out + fpair[...].astype(F32)
    fhalf[...] = out.astype(BF16)
    for d in (2, 1, 3):
        send(fhalf, frecv.at[d - 1], f_sem.at[d], e, at_y(d))
    mine = pl.ds(pl.multiple_of(x * 128, 128), 128)
    out = out + rall[pl.ds(c * 4, 4), :, :, mine].reshape(256, 128).astype(F32)
    for d in (1, 3, 2):
        arrived(frecv.at[d - 1], f_sem.at[d])
        out = out + frecv[d - 1].astype(F32)
    mgath[c] = out.astype(BF16)
    send(mgath.at[c], mgath.at[c], m_sem.at[0], e, partner)
    arrived(mgath.at[1 - c], m_sem.at[0])
    mixed[...] = mgath[...].reshape(SEQS, 128)
    for copy in started:
        copy.wait_send()


def finish_kernel(a, b, c, a_out, b_out, c_out):
    a_out[...] = a[...]
    b_out[...] = b[...]
    c_out[...] = c[...]


def per_device(
    stream, norm_gain, w_query, w_key, w_value, break_offset, cache_keys, cache_values, lengths, w_output, head_gain,
    ffn_gain, route_experts, route_weights, expert_gate, expert_up, expert_down, dense_gate, dense_up, dense_down, mix_gain,
):
    any_spec = pl.BlockSpec(memory_space=pl.ANY)
    vm = pl.BlockSpec(memory_space=pltpu.VMEM)
    dma = pltpu.SemaphoreType.DMA

    def b(*shape):
        return pltpu.VMEM(shape, BF16)

    def f(*shape):
        return pltpu.VMEM(shape, F32)

    scratch = dict(
        ngain=f(1, 128), hgain=f(2, 128), fgain=f(1, 128), mgain=f(1, 128),
        route=pltpu.VMEM((2, SEQS), jnp.int32), rweights=f(2, SEQS), boff=pltpu.SMEM((2,), F32), lens=pltpu.SMEM((ROWS,), jnp.int32),
        strm=b(NX, NZ, ROWS, 128), wqkv=b(128, 512), kbuf=b(ROWS, LEN, 128), vbuf=b(ROWS, LEN, 128),
        xgain=b(NX, 128, 128), yq=b(NX, NZ, ROWS, 256), yqr=b(NX - 1, NZ, ROWS, 256),
        yk=b(NX, NZ, ROWS, 256), ykr=b(NX - 1, NZ, ROWS, 256), ssq=f(NX, 8, 128), ssqr=f(NX - 1, 8, 128),
        zq=b(NZ - 1, ROWS, 256), zqr=b(NZ - 1, ROWS, 256), zk=b(NZ, ROWS, 256), zkr=b(NZ - 1, ROWS, 256),
        zsq=f(8, 128), zsqr=f(NZ - 1, 8, 128),
        wog=b(NX, 256, 128), hall=b(NZ, ROWS, 256), obuf=b(NZ, ROWS, 512), orecv=b(NT - 1, ROWS, 512),
        sres=b(NX, ROWS, 128), fgb=f(8, 128), fgall=f(NX, 8, 128),
        wgu=b(NX, 128, 256), ddb=b(512, 128), egb=b(NZ, 512, 128), eub=b(NZ, 512, 128), edb=b(NZ, 128, 512),
        pmat=b(64, SEQS), ctm=b(256, SEQS), rbuf=b(ROWS, 512), rall=b(NT, NX, ROWS, 512), gbuf=b(SEQS, 512),
        fsq=f(8, 128), fsqr=f(NZ - 1, 8, 128), gub=b(NZ, 64, 256), gurecv=b(NZ - 1, 64, 256),
        dbuf=b(NZ, 8, 512), xe=b(NT, NZ, 8, 512), hd=b(NX, NZ, 64, 128),
        pown=b(NZ, NX, HALF, 128), pout=b(NZ, NX, HALF, 128), precv=b(NZ, NX, HALF, 128), rsum=b(NZ, 4, HALF, 128),
        ysum=b(3, NZ, HALF, 128), back=b(NZ, NX, 8, 128), rt=b(32, 8, 128), fbuf=b(2, 256, 128), fpair=b(256, 128), fhalf=b(256, 128), frecv=b(3, 256, 128), mgath=b(2, 256, 128),
        lsem=dma((32,)), ssem=dma((320,)), ring_sem=pltpu.SemaphoreType.REGULAR((4,)),
        yq_sem=dma((24,)), yk_sem=dma((3,)), sx_sem=dma((3,)), wo_sem=dma((3,)), wg_sem=dma((3,)), wu_sem=dma((3,)),
        sr_sem=dma((3,)), fg_sem=dma((3,)), zq_sem=dma((7,)), zk_sem=dma((7,)), sz_sem=dma((7,)), h_sem=dma((7,)), o_sem=dma((7,)),
        r_sem=dma((16,)), rf_sem=dma((16,)),
        fs_sem=dma((7,)), gu_sem=dma((7,)), d_sem=dma((7,)), xy_sem=dma((24,)), xe_sem=dma((32,)), hz_sem=dma((7,)),
        hx_sem=dma((24,)), p_sem=dma((8,)), ys_sem=dma((24,)), rt_sem=dma((32,)), f_sem=dma((4,)), m_sem=dma((1,)),
    )
    results = pl.pallas_call(
        step_kernel,
        name="step",
        out_shape=(
            jax.ShapeDtypeStruct((SEQS, 128), BF16),
            jax.ShapeDtypeStruct((ROWS, 128), BF16),
            jax.ShapeDtypeStruct((ROWS, 128), BF16),
        ),
        in_specs=[any_spec] * 21,
        out_specs=(vm, vm, vm),
        scratch_shapes=list(scratch.values()),
        compiler_params=pltpu.CompilerParams(collective_id=0, has_side_effects=True, vmem_limit_bytes=60 * 1024 * 1024),
    )(
        stream.reshape(NZ, NX, ROWS, 128), w_query, w_key, w_value,
        cache_keys.reshape(ROWS, LEN, 128), cache_values.reshape(ROWS, LEN, 128), w_output,
        expert_gate.reshape(NZ, 512, 128), expert_up.reshape(NZ, 512, 128), expert_down.reshape(128, MODEL),
        dense_gate, dense_up, dense_down,
        norm_gain.reshape(1, 128), head_gain.reshape(2, 128), ffn_gain.reshape(1, 128), mix_gain.reshape(1, 128),
        route_experts.T, route_weights.T, break_offset, lengths,
    )
    return pl.pallas_call(
        finish_kernel,
        name="finish",
        out_shape=tuple(jax.ShapeDtypeStruct(r.shape, r.dtype) for r in results),
        in_specs=[vm] * 3,
        out_specs=(vm,) * 3,
    )(*results)


def solution(mesh):
    in_specs = (
        P(None, "ep"),
        P("ep"),
        P("ep", "tp"),
        P("ep", "tp"),
        P("ep", "tp"),
        P("tp"),
        P("ep", None, "tp", None),
        P("ep", None, "tp", None),
        P("ep"),
        P("tp", "ep"),
        P("tp"),
        P("ep"),
        P(),
        P(),
        P("ep", None, "tp"),
        P("ep", None, "tp"),
        P("ep", "tp", None),
        P("ep", "tp"),
        P("ep", "tp"),
        P("tp", "ep"),
        P("ep"),
    )
    out_specs = (P(None, "ep"), P("ep", "tp"), P("ep", "tp"))
    return jax.shard_map(
        per_device, mesh=mesh, in_specs=in_specs, out_specs=out_specs, check_vma=False
    )
```

```python
import jax
import jax.numpy as jnp
from jax import lax
from jax.experimental import pallas as pl
from jax.experimental.pallas import tpu as pltpu
from jax.sharding import PartitionSpec as P

EPSILON = 1e-06
NX, NZ, NT = 4, 8, 8
MODEL, HD, LEN, ROWS, SEQS = 4096, 128, 1024, 16, 512
CAP, HALF = 64, 32
F32, BF16 = jnp.float32, jnp.bfloat16
HIGH = lax.Precision.HIGHEST
MESH = pl.DeviceIdType.MESH
FAR_FIRST = (4, 3, 5, 2, 6, 1, 7)
NEAR_FIRST = (1, 7, 2, 6, 3, 5, 4)


def iota(shape, dim):
    return lax.broadcasted_iota(jnp.int32, shape, dim)


def step_kernel(
    stream, wq, wk, wv, ck, cv, wo, eg, eu, ed, dg, du, dd,
    ngain_hbm, hgain_hbm, fgain_hbm, mgain_hbm, route_hbm, rweights_hbm, boff_hbm, lens_hbm,
    mixed, key_rows, value_rows,
    ngain, hgain, fgain, mgain, route, rweights, boff, lens,
    strm, wqkv, kbuf, vbuf, xgain, yq, yqr, yk, ykr, ssq, ssqr, zq, zqr, zk, zkr, zsq, zsqr,
    wog, hall, obuf, orecv, sres, fgb, fgall, wgu, ddb, egb, eub, edb,
    pmat, ctm, rbuf, rall, gbuf, fsq, fsqr, gub, gurecv, dbuf, xe, hd,
    pown, pout, precv, rsum, ysum, back, rt, fbuf, fpair, fhalf, frecv, mgath, kvout,
    lsem, ssem, ring_sem,
    yq_sem, yk_sem, sx_sem, wo_sem, wg_sem, wu_sem, sr_sem, fg_sem, zq_sem, zk_sem, sz_sem, h_sem, o_sem, r_sem, rf_sem,
    fs_sem, gu_sem, d_sem, xy_sem, xe_sem, hz_sem, hx_sem, p_sem, ys_sem, rt_sem, f_sem, m_sem,
):
    e = lax.axis_index("ep")
    t = lax.axis_index("tp")
    z = lax.div(e, NX)
    x = lax.rem(e, NX)
    c = lax.rem(t, 2)
    partner = t + 1 - 2 * c

    def at_x(d):
        return lax.rem(x + d, NX)

    def at_z(d):
        return lax.rem(z + d, NZ)

    def at_t(d):
        return lax.rem(t + d, NT)

    started = []

    def send(src, dst, rsem, dev_e, dev_t):
        copy = pltpu.make_async_remote_copy(
            src_ref=src, dst_ref=dst, send_sem=ssem.at[len(started)], recv_sem=rsem,
            device_id=(dev_e, dev_t), device_id_type=MESH,
        )
        copy.start()
        started.append(copy)

    def arrived(dst, rsem):
        pltpu.make_async_copy(dst, dst, rsem).wait()

    loads = []

    def load(src, dst):
        copy = pltpu.make_async_copy(src, dst, lsem.at[len(loads)])
        copy.start()
        loads.append(copy)
        return copy

    def columns(ref, block):
        return ref.at[:, pl.ds(pl.multiple_of(block * 128, 128), 128)]

    def signal(sem, dev_e, dev_t):
        pl.semaphore_signal(sem, inc=1, device_id=(dev_e, dev_t), device_id_type=MESH)

    barrier = pltpu.get_barrier_semaphore()
    for d in (1, NZ - 1):
        signal(barrier, at_z(d) * NX + x, t)
    for d in range(1, NX):
        signal(barrier, z * NX + at_x(d), t)
    for d in range(1, NT):
        signal(barrier, e, at_t(d))

    c_s = [load(stream.at[:, xi], strm.at[xi]) for xi in range(NX)]
    c_w = [load(ngain_hbm, ngain), load(wq, wqkv.at[:, 0:256]), load(wk, wqkv.at[:, 256:384]), load(wv, wqkv.at[:, 384:512])]
    c_route = [load(route_hbm, route), load(rweights_hbm, rweights)]
    c_small = [load(hgain_hbm, hgain), load(mgain_hbm, mgain), load(boff_hbm, boff), load(lens_hbm, lens)]
    c_fg = load(fgain_hbm, fgain)
    c_wo = load(wo, wog.at[x])
    c_k = load(ck, kbuf)
    c_v = load(cv, vbuf)
    c_dg = load(columns(dg, x), wgu.at[x, :, 0:128])
    c_du = load(columns(du, x), wgu.at[x, :, 128:256])
    c_dd = load(dd, ddb)
    c_eg = load(eg, egb)
    c_eu = load(eu, eub)
    c_ed = [load(ed.at[:, zi * 512 : (zi + 1) * 512], edb.at[zi]) for zi in range(NZ)]

    for copy in c_s + c_w:
        copy.wait()
    gain = ngain[...]
    w = wqkv[...]
    for xi in range(NX):
        rows = strm[xi].reshape(NZ * ROWS, HD).astype(F32)
        scaled = (rows * gain).astype(BF16)
        xgain[xi] = scaled
        yq[xi] = jnp.dot(scaled, w[:, 0:256], preferred_element_type=F32).astype(BF16).reshape(NZ, ROWS, 256)
        sums = jnp.sum((rows * rows).T, axis=0, keepdims=True)
        ssq[xi] = jnp.broadcast_to(sums, (8, HD))
    c_fg.wait()
    fgb[...] = jnp.broadcast_to(fgain[...], (8, HD))

    pl.semaphore_wait(barrier, 2 + NX - 1 + NT - 1)

    for d in (2, 1, 3):
        send(ssq.at[at_x(d)], ssqr.at[d - 1], sx_sem.at[d - 1], z * NX + at_x(d), t)
    for k in FAR_FIRST + (0,):
        for d in (2, 1, 3):
            send(yq.at[at_x(d), at_z(k)], yqr.at[d - 1, k], yq_sem.at[k * 3 + d - 1], z * NX + at_x(d), t)
    signal(ring_sem.at[0], at_z(1) * NX + x, t)
    signal(ring_sem.at[1], at_z(7) * NX + x, t)
    c_wo.wait()
    for d in (2, 1, 3):
        to = z * NX + at_x(d)
        send(wog.at[x], wog.at[x], wo_sem.at[d - 1], to, t)
        send(strm.at[at_x(d), t], sres.at[x], sr_sem.at[d - 1], to, t)
        send(fgb, fgall.at[x], fg_sem.at[d - 1], to, t)
    sres[x] = strm[x, t]
    fgall[x] = fgb[...]
    pl.semaphore_wait(ring_sem.at[0], 1)
    pl.semaphore_wait(ring_sem.at[1], 1)
    signal(ring_sem.at[2], at_z(2) * NX + x, t)
    signal(ring_sem.at[3], at_z(6) * NX + x, t)
    for xi in range(NX):
        yk[xi] = jnp.dot(xgain[xi], w[:, 256:512], preferred_element_type=F32).astype(BF16).reshape(NZ, ROWS, 256)
    for d in (2, 1, 3):
        send(yk.at[at_x(d)], ykr.at[d - 1], yk_sem.at[d - 1], z * NX + at_x(d), t)
    for d in (2, 1, 3):
        to = z * NX + at_x(d)
        send(columns(dg, at_x(d)), wgu.at[x, :, 0:128], wg_sem.at[d - 1], to, t)
        send(columns(du, at_x(d)), wgu.at[x, :, 128:256], wu_sem.at[d - 1], to, t)
    pl.semaphore_wait(ring_sem.at[2], 1)
    pl.semaphore_wait(ring_sem.at[3], 1)

    sq = ssq[x]
    for d in (1, 3, 2):
        arrived(ssqr.at[d - 1], sx_sem.at[d - 1])
        sq = sq + ssqr[d - 1]
    zsq[...] = sq
    for d in FAR_FIRST:
        send(zsq, zsqr.at[d - 1], sz_sem.at[d - 1], at_z(d) * NX + x, t)
    for k in FAR_FIRST + (0,):
        total = yq[x, at_z(k)].astype(F32)
        for d in (1, 3, 2):
            arrived(yqr.at[d - 1, k], yq_sem.at[k * 3 + d - 1])
            total = total + yqr[d - 1, k].astype(F32)
        if k:
            zq[k - 1] = total.astype(BF16)
            send(zq.at[k - 1], zqr.at[k - 1], zq_sem.at[k - 1], at_z(k) * NX + x, t)
        else:
            queries = total

    for copy in c_route:
        copy.wait()
    names = [route[0:1], route[1:2]]
    expert = iota((32, SEQS), 0)
    chosen = (jnp.where(names[0] == expert, 1.0, 0.0) + jnp.where(names[1] == expert, 1.0, 0.0)).astype(BF16)
    before = jnp.where(iota((SEQS, SEQS), 0) < iota((SEQS, SEQS), 1), 1.0, 0.0).astype(BF16)
    earlier = jnp.dot(chosen, before, preferred_element_type=F32)
    slots = [
        n * CAP + jnp.sum(jnp.where(n == expert, earlier, 0.0), axis=0, keepdims=True).astype(jnp.int32) for n in names
    ]
    weight_sum = rweights[0:1] + rweights[1:2]
    shares = [rweights[0:1] / weight_sum, rweights[1:2] / weight_sum]
    y = lax.div(t, 2)
    row = iota((64, SEQS), 0)
    slot = lax.shift_right_logical(row, 3) * (NX * CAP) + (x * CAP + c * HALF + y * 8) + (row & 7)
    pmat[...] = jnp.where((slots[0] == slot) | (slots[1] == slot), 1.0, 0.0).astype(BF16)
    for i in range(2):
        row = iota((128, SEQS), 0) + i * 128
        slot = lax.shift_right_logical(row, 3) * CAP + c * HALF + y * 8 + (row & 7)
        ctm[i * 128 : (i + 1) * 128] = jnp.where(
            slots[0] == slot, shares[0], jnp.where(slots[1] == slot, shares[1], 0.0)
        ).astype(BF16)

    sq = zsq[...]
    for d in NEAR_FIRST:
        arrived(zqr.at[d - 1], zq_sem.at[d - 1])
        arrived(zsqr.at[d - 1], sz_sem.at[d - 1])
        queries = queries + zqr[d - 1].astype(F32)
        sq = sq + zsqr[d - 1]
    lane = iota((ROWS, HD), 1)
    pick = lane == z * ROWS + iota((ROWS, HD), 0)
    mean = jnp.sum(jnp.where(pick, jnp.broadcast_to(sq[0:1], (ROWS, HD)), 0.0), axis=1, keepdims=True) / MODEL
    token_scale = lax.rsqrt(mean + EPSILON)
    queries = queries * token_scale

    q = jnp.concatenate([queries[:, 0:128], queries[:, 128:256]], axis=0).astype(BF16).astype(F32)
    seq = lax.rem(iota((2 * ROWS, 1), 0), ROWS)
    c_k.wait()
    scores = jnp.zeros((2 * ROWS, LEN), F32)
    for p in range(ROWS // 2):
        keys = jnp.concatenate([kbuf[2 * p], kbuf[2 * p + 1]], axis=1)
        own = jnp.concatenate([jnp.where(seq == 2 * p, q, 0.0), jnp.where(seq == 2 * p + 1, q, 0.0)], axis=1)
        scores = scores + lax.dot_general(own.astype(BF16), keys, (((1,), (1,)), ((), ())), preferred_element_type=F32)
    first = iota((2 * ROWS, 1), 0) < ROWS
    for copy in c_small:
        copy.wait()
    length = jnp.zeros((2 * ROWS, 1), jnp.int32)
    for s in range(ROWS):
        length = jnp.where(seq == s, lens[s], length)
    scores = scores * HD ** (-0.5) + jnp.where(first, boff[0], boff[1])
    inside = iota((2 * ROWS, LEN), 1) < length
    tail = jnp.log1p(jnp.exp(-jnp.abs(scores)))
    failed = jnp.where(inside, -(jnp.maximum(scores, 0.0) + tail), 0.0)
    blocks = [failed[:, b * 128 : (b + 1) * 128] for b in range(LEN // 128)]
    later = (iota((128, 128), 0) > iota((128, 128), 1)).astype(F32)
    within = jnp.dot(jnp.concatenate(blocks, axis=0), later, precision=HIGH, preferred_element_type=F32)
    after = jnp.zeros((2 * ROWS, 1), F32)
    sums = []
    for b in reversed(range(LEN // 128)):
        sums.insert(0, within[b * 32 : (b + 1) * 32] + after)
        after = after + jnp.sum(blocks[b], axis=1, keepdims=True)
    later_sum = jnp.concatenate(sums, axis=1)
    weights = jnp.where(inside, jnp.exp(jnp.minimum(scores, 0.0) - tail + later_sum), 0.0).astype(BF16)
    c_v.wait()
    attended = jnp.zeros((2 * ROWS, HD), F32)
    for p in range(ROWS // 2):
        vals = jnp.concatenate([vbuf[2 * p], vbuf[2 * p + 1]], axis=1)
        both = jnp.dot(weights, vals, preferred_element_type=F32)
        attended = jnp.where(seq == 2 * p, both[:, 0:128], jnp.where(seq == 2 * p + 1, both[:, 128:256], attended))
    norm = lax.rsqrt(jnp.mean(attended * attended, axis=1, keepdims=True) + EPSILON)
    head = attended * norm * jnp.where(first, hgain[0:1], hgain[1:2])
    hall[z] = jnp.concatenate([head[:ROWS], head[ROWS:]], axis=1).astype(BF16)

    for d in FAR_FIRST:
        send(hall.at[z], hall.at[z], h_sem.at[d - 1], at_z(d) * NX + x, t)
    kv = yk[x].astype(F32)
    for d in (1, 3, 2):
        arrived(ykr.at[d - 1], yk_sem.at[d - 1])
        kv = kv + ykr[d - 1].astype(F32)
    zk[...] = kv.astype(BF16)
    for d in FAR_FIRST:
        send(zk.at[at_z(d)], zkr.at[d - 1], zk_sem.at[d - 1], at_z(d) * NX + x, t)
    for d in (1, 2, 3):
        arrived(wog.at[at_x(NX - d)], wo_sem.at[d - 1])
        arrived(sres.at[at_x(NX - d)], sr_sem.at[d - 1])
        arrived(fgall.at[at_x(NX - d)], fg_sem.at[d - 1])
        arrived(wgu.at[at_x(NX - d), :, 0:128], wg_sem.at[d - 1])
        arrived(wgu.at[at_x(NX - d), :, 128:256], wu_sem.at[d - 1])
    c_dg.wait()
    c_du.wait()
    for d in NEAR_FIRST:
        arrived(hall.at[at_z(NZ - d)], h_sem.at[d - 1])
    heads = hall[...].reshape(NZ * ROWS, 256)
    for xi in range(NX):
        part = jnp.dot(heads, wog[xi], preferred_element_type=F32)
        obuf[:, :, xi * 128 : (xi + 1) * 128] = part.astype(BF16).reshape(NZ, ROWS, 128)
    for d in (4, 5, 3, 2, 6, 7, 1):
        send(obuf.at[at_t(d)], orecv.at[d - 1], o_sem.at[d - 1], e, at_t(d))
    attn = obuf[t].astype(F32)
    for d in NEAR_FIRST:
        arrived(orecv.at[d - 1], o_sem.at[d - 1])
        attn = attn + orecv[d - 1].astype(F32)
    attn = attn.astype(BF16)
    rbuf[...] = (attn.astype(F32) + jnp.concatenate([sres[xi].astype(F32) for xi in range(NX)], axis=1)).astype(BF16)

    def at_y(d):
        return lax.rem(t + 2 * d, NT)

    for dy in (2, 1, 3, 0):
        for dx in (2, 1, 3, 0):
            if dy or dx:
                send(rbuf, rall.at[t, x], r_sem.at[dy * NX + dx], z * NX + at_x(dx), at_y(dy))
    send(rbuf, rall.at[t, x], rf_sem.at[0], e, partner)
    rall[t, x] = rbuf[...]
    kv = zk[z].astype(F32)
    for d in NEAR_FIRST:
        arrived(zkr.at[d - 1], zk_sem.at[d - 1])
        kv = kv + zkr[d - 1].astype(F32)
    kv = kv * token_scale
    kvout[0] = kv[:, 0:128].astype(BF16)
    kvout[1] = kv[:, 128:256].astype(BF16)
    c_out = [load(kvout.at[0], key_rows), load(kvout.at[1], value_rows)]
    for dy in (0, 1, 3, 2):
        for dx in (0, 1, 3, 2):
            if dy or dx:
                block = rall.at[at_y(4 - dy), at_x(NX - dx)]
                arrived(block, r_sem.at[dy * NX + dx])
                send(block, block, rf_sem.at[dy * NX + dx], e, partner)
    other = lax.div(t, 2) * 2 + 1 - c
    for dy in range(4):
        for dx in range(NX):
            arrived(rall.at[lax.rem(other + 2 * (4 - dy), NT), at_x(NX - dx)], rf_sem.at[dy * NX + dx])
    gains = jnp.concatenate([fgall[xi][0:1] for xi in range(NX)], axis=1)
    for i in range(4):
        rows = rall[2 * i : 2 * i + 2].reshape(128, 512).astype(F32)
        gbuf[i * 128 : (i + 1) * 128] = (rows * gains).astype(BF16)
    dispatched = jnp.dot(pmat[...], gbuf[...], preferred_element_type=F32)
    dbuf[...] = dispatched.reshape(NZ, 8, 512).astype(BF16)
    for d in FAR_FIRST:
        send(dbuf.at[at_z(d)], xe.at[t, z], d_sem.at[d - 1], at_z(d) * NX + x, t)
    xe[t, z] = dbuf[z]
    square_rows = []
    for i in range(4):
        rows = rall[2 * i : 2 * i + 2].reshape(128, 512).astype(F32)
        squares = rows * rows
        squares = squares[:, 0:128] + squares[:, 128:256] + squares[:, 256:384] + squares[:, 384:512]
        square_rows.append(jnp.sum(squares.T, axis=0, keepdims=True))
    fsq[...] = jnp.concatenate(square_rows + [jnp.zeros((4, 128), F32)], axis=0)
    for d in FAR_FIRST:
        send(fsq, fsqr.at[d - 1], fs_sem.at[d - 1], at_z(d) * NX + x, t)
    wide = wgu[...].reshape(512, 256)
    for i in range(4):
        part = jnp.dot(gbuf[i * 128 : (i + 1) * 128], wide, preferred_element_type=F32)
        gub[2 * i : 2 * i + 2] = part.astype(BF16).reshape(2, 64, 256)
    for d in FAR_FIRST:
        send(gub.at[at_z(d)], gurecv.at[d - 1], gu_sem.at[d - 1], at_z(d) * NX + x, t)

    def spread(d):
        block = xe.at[t, at_z(NZ - d)]
        if d:
            arrived(block, d_sem.at[d - 1])
        for dy in (2, 1, 3):
            send(block, block, xy_sem.at[d * 3 + dy - 1], e, at_y(dy))
        send(block, block, xe_sem.at[d * 4], e, partner)

    for d in (0,) + NEAR_FIRST:
        spread(d)
    sq = fsq[...]
    for d in NEAR_FIRST:
        arrived(fsqr.at[d - 1], fs_sem.at[d - 1])
        sq = sq + fsqr[d - 1]
    inverse = lax.rsqrt(sq / MODEL + EPSILON)
    inverse = jnp.concatenate([inverse[i : i + 1] for i in range(4)], axis=1)
    slot = iota((CAP, SEQS), 0) + e * CAP
    mine = (slots[0] == slot) | (slots[1] == slot)
    slot_scale = jnp.sum(jnp.where(mine, jnp.broadcast_to(inverse, (CAP, SEQS)), 0.0), axis=1, keepdims=True)
    own_row = iota((64, SEQS), 1) == iota((64, SEQS), 0) + z * 64
    row_scale = jnp.sum(jnp.where(own_row, jnp.broadcast_to(inverse, (64, SEQS)), 0.0), axis=1, keepdims=True)
    c_eg.wait()
    c_eu.wait()
    def product(core, zs):
        rows = jnp.concatenate([xe[2 * yi + core, zs].astype(F32) for yi in range(4)], axis=0).astype(BF16)
        both = jnp.concatenate([egb[zs], eub[zs]], axis=1)
        return jnp.dot(rows, both, preferred_element_type=F32)

    near = jnp.zeros((HALF, 256), F32)
    for d in (0,) + NEAR_FIRST:
        zs = at_z(NZ - d)
        for dy in (1, 3, 2):
            block = xe.at[at_y(4 - dy), zs]
            arrived(block, xy_sem.at[d * 3 + dy - 1])
            send(block, block, xe_sem.at[d * 4 + dy], e, partner)
        near = near + product(c, zs)

    gu = gub[z].astype(F32)
    for d in NEAR_FIRST:
        arrived(gurecv.at[d - 1], gu_sem.at[d - 1])
        gu = gu + gurecv[d - 1].astype(F32)
    gu = gu * row_scale
    gate = gu[:, 0:128]
    hd[x, z] = (gate / (1.0 + jnp.exp(-gate)) * gu[:, 128:256]).astype(BF16)
    for d in FAR_FIRST:
        send(hd.at[x, z], hd.at[x, z], hz_sem.at[d - 1], at_z(d) * NX + x, t)

    across = jnp.zeros((HALF, 256), F32)
    for d in (0,) + NEAR_FIRST:
        zs = at_z(NZ - d)
        for dy in (0, 1, 3, 2):
            arrived(xe.at[lax.rem(partner + 2 * (4 - dy), NT), zs], xe_sem.at[d * 4 + dy])
        across = across + product(1 - c, zs)
    acc = jnp.concatenate([jnp.where(c == 0, near, across), jnp.where(c == 0, across, near)], axis=0)
    acc = acc * slot_scale
    gate = acc[:, 0:128]
    hidden = (gate / (1.0 + jnp.exp(-gate)) * acc[:, 128:256]).astype(BF16)
    for copy in c_ed:
        copy.wait()
    for k, d in enumerate(FAR_FIRST + (0,)):
        zi = at_z(d)
        part = jnp.dot(hidden, edb[zi], preferred_element_type=F32)
        kept = jnp.where(c == 0, part[:HALF], part[HALF:]).astype(BF16)
        given = jnp.where(c == 0, part[HALF:], part[:HALF]).astype(BF16)
        for xi in range(NX):
            pown[zi, xi] = kept[:, xi * 128 : (xi + 1) * 128]
            pout[zi, xi] = given[:, xi * 128 : (xi + 1) * 128]
        send(pout.at[zi], precv.at[zi], p_sem.at[k], e, partner)

    for k, d in enumerate(FAR_FIRST + (0,)):
        zi = at_z(d)
        arrived(precv.at[zi], p_sem.at[k])
        pair = pown[zi].astype(F32) + precv[zi].astype(F32)
        for yi in range(4):
            rsum[zi, yi] = jnp.concatenate([pair[xi, yi * 8 : (yi + 1) * 8] for xi in range(NX)], axis=0).astype(BF16)
        for dy in (2, 1, 3):
            send(rsum.at[zi, lax.rem(y + dy, 4)], ysum.at[dy - 1, zi], ys_sem.at[k * 3 + dy - 1], e, at_y(dy))

    def onward(d):
        block = hd.at[x, at_z(NZ - d)]
        if d:
            arrived(block, hz_sem.at[d - 1])
        for dx in (2, 1, 3):
            send(block, block, hx_sem.at[d * 3 + dx - 1], z * NX + at_x(dx), t)

    for d in (0, 1, 7, 2, 6):
        onward(d)
    for k, d in enumerate(FAR_FIRST + (0,)):
        zi = at_z(d)
        whole = rsum[zi, y].astype(F32)
        for dy in (1, 3, 2):
            arrived(ysum.at[dy - 1, zi], ys_sem.at[k * 3 + dy - 1])
            whole = whole + ysum[dy - 1, zi].astype(F32)
        for xi in range(NX):
            back[zi, xi] = whole[xi * 8 : (xi + 1) * 8].astype(BF16)
        for dx in (2, 1, 3, 0):
            if d or dx:
                send(back.at[zi, at_x(dx)], rt.at[e], rt_sem.at[d * NX + dx], zi * NX + at_x(dx), t)
    rt[e] = back[z, x]
    for d in (3, 5, 4):
        onward(d)

    for d in range(NZ):
        for dx in range(NX):
            if d or dx:
                arrived(rt.at[at_z(NZ - d) * NX + at_x(NX - dx)], rt_sem.at[d * NX + dx])
    returned = rt[...].astype(F32).reshape(256, 128).astype(BF16)
    moe = lax.dot_general(ctm[...], returned, (((0,), (0,)), ((), ())), preferred_element_type=F32)
    for d in (0,) + NEAR_FIRST:
        for dx in (1, 3, 2):
            arrived(hd.at[at_x(NX - dx), at_z(NZ - d)], hx_sem.at[d * 3 + dx - 1])
    c_dd.wait()
    dense = jnp.zeros((SEQS, 128), F32)
    for xi in range(NX):
        dense = dense + jnp.dot(hd[xi].reshape(SEQS, 128), ddb[xi * 128 : (xi + 1) * 128], preferred_element_type=F32)
    fbuf[...] = (moe + mgain[...] * dense).astype(BF16).reshape(2, 256, 128)

    send(fbuf.at[1 - c], fpair, f_sem.at[0], e, partner)
    out = fbuf[c].astype(F32)
    arrived(fpair, f_sem.at[0])
    out = out + fpair[...].astype(F32)
    fhalf[...] = out.astype(BF16)
    for d in (2, 1, 3):
        send(fhalf, frecv.at[d - 1], f_sem.at[d], e, at_y(d))
    mine = pl.ds(pl.multiple_of(x * 128, 128), 128)
    out = out + rall[pl.ds(c * 4, 4), :, :, mine].reshape(256, 128).astype(F32)
    for d in (1, 3, 2):
        arrived(frecv.at[d - 1], f_sem.at[d])
        out = out + frecv[d - 1].astype(F32)
    mgath[...] = out.astype(BF16)
    send(mgath, mixed.at[c], m_sem.at[0], e, partner)
    c_out.append(load(mgath, mixed.at[c]))
    arrived(mixed.at[1 - c], m_sem.at[0])
    for copy in c_out:
        copy.wait()
    for copy in started:
        copy.wait_send()


def finish_kernel(a, b, c, a_out, b_out, c_out):
    a_out[...] = a[...]
    b_out[...] = b[...]
    c_out[...] = c[...]


def per_device(
    stream, norm_gain, w_query, w_key, w_value, break_offset, cache_keys, cache_values, lengths, w_output, head_gain,
    ffn_gain, route_experts, route_weights, expert_gate, expert_up, expert_down, dense_gate, dense_up, dense_down, mix_gain,
):
    any_spec = pl.BlockSpec(memory_space=pl.ANY)
    vm = pl.BlockSpec(memory_space=pltpu.VMEM)
    dma = pltpu.SemaphoreType.DMA

    def b(*shape):
        return pltpu.VMEM(shape, BF16)

    def f(*shape):
        return pltpu.VMEM(shape, F32)

    scratch = dict(
        ngain=f(1, 128), hgain=f(2, 128), fgain=f(1, 128), mgain=f(1, 128),
        route=pltpu.VMEM((2, SEQS), jnp.int32), rweights=f(2, SEQS), boff=pltpu.SMEM((2,), F32), lens=pltpu.SMEM((ROWS,), jnp.int32),
        strm=b(NX, NZ, ROWS, 128), wqkv=b(128, 512), kbuf=b(ROWS, LEN, 128), vbuf=b(ROWS, LEN, 128),
        xgain=b(NX, 128, 128), yq=b(NX, NZ, ROWS, 256), yqr=b(NX - 1, NZ, ROWS, 256),
        yk=b(NX, NZ, ROWS, 256), ykr=b(NX - 1, NZ, ROWS, 256), ssq=f(NX, 8, 128), ssqr=f(NX - 1, 8, 128),
        zq=b(NZ - 1, ROWS, 256), zqr=b(NZ - 1, ROWS, 256), zk=b(NZ, ROWS, 256), zkr=b(NZ - 1, ROWS, 256),
        zsq=f(8, 128), zsqr=f(NZ - 1, 8, 128),
        wog=b(NX, 256, 128), hall=b(NZ, ROWS, 256), obuf=b(NZ, ROWS, 512), orecv=b(NT - 1, ROWS, 512),
        sres=b(NX, ROWS, 128), fgb=f(8, 128), fgall=f(NX, 8, 128),
        wgu=b(NX, 128, 256), ddb=b(512, 128), egb=b(NZ, 512, 128), eub=b(NZ, 512, 128), edb=b(NZ, 128, 512),
        pmat=b(64, SEQS), ctm=b(256, SEQS), rbuf=b(ROWS, 512), rall=b(NT, NX, ROWS, 512), gbuf=b(SEQS, 512),
        fsq=f(8, 128), fsqr=f(NZ - 1, 8, 128), gub=b(NZ, 64, 256), gurecv=b(NZ - 1, 64, 256),
        dbuf=b(NZ, 8, 512), xe=b(NT, NZ, 8, 512), hd=b(NX, NZ, 64, 128),
        pown=b(NZ, NX, HALF, 128), pout=b(NZ, NX, HALF, 128), precv=b(NZ, NX, HALF, 128), rsum=b(NZ, 4, HALF, 128),
        ysum=b(3, NZ, HALF, 128), back=b(NZ, NX, 8, 128), rt=b(32, 8, 128), fbuf=b(2, 256, 128), fpair=b(256, 128), fhalf=b(256, 128), frecv=b(3, 256, 128), mgath=b(256, 128), kvout=b(2, ROWS, 128),
        lsem=dma((40,)), ssem=dma((320,)), ring_sem=pltpu.SemaphoreType.REGULAR((4,)),
        yq_sem=dma((24,)), yk_sem=dma((3,)), sx_sem=dma((3,)), wo_sem=dma((3,)), wg_sem=dma((3,)), wu_sem=dma((3,)),
        sr_sem=dma((3,)), fg_sem=dma((3,)), zq_sem=dma((7,)), zk_sem=dma((7,)), sz_sem=dma((7,)), h_sem=dma((7,)), o_sem=dma((7,)),
        r_sem=dma((16,)), rf_sem=dma((16,)),
        fs_sem=dma((7,)), gu_sem=dma((7,)), d_sem=dma((7,)), xy_sem=dma((24,)), xe_sem=dma((32,)), hz_sem=dma((7,)),
        hx_sem=dma((24,)), p_sem=dma((8,)), ys_sem=dma((24,)), rt_sem=dma((32,)), f_sem=dma((4,)), m_sem=dma((1,)),
    )
    results = pl.pallas_call(
        step_kernel,
        name="step",
        out_shape=(
            jax.ShapeDtypeStruct((2, 256, 128), BF16),
            jax.ShapeDtypeStruct((ROWS, 128), BF16),
            jax.ShapeDtypeStruct((ROWS, 128), BF16),
        ),
        in_specs=[any_spec] * 21,
        out_specs=(any_spec,) * 3,
        scratch_shapes=list(scratch.values()),
        compiler_params=pltpu.CompilerParams(collective_id=0, has_side_effects=True, vmem_limit_bytes=60 * 1024 * 1024),
    )(
        stream.reshape(NZ, NX, ROWS, 128), w_query, w_key, w_value,
        cache_keys.reshape(ROWS, LEN, 128), cache_values.reshape(ROWS, LEN, 128), w_output,
        expert_gate.reshape(NZ, 512, 128), expert_up.reshape(NZ, 512, 128), expert_down.reshape(128, MODEL),
        dense_gate, dense_up, dense_down,
        norm_gain.reshape(1, 128), head_gain.reshape(2, 128), ffn_gain.reshape(1, 128), mix_gain.reshape(1, 128),
        route_experts.T, route_weights.T, break_offset, lengths,
    )
    results = (results[0].reshape(SEQS, 128), results[1], results[2])
    return pl.pallas_call(
        finish_kernel,
        name="finish",
        out_shape=tuple(jax.ShapeDtypeStruct(r.shape, r.dtype) for r in results),
        in_specs=[vm] * 3,
        out_specs=(vm,) * 3,
    )(*results)


def solution(mesh):
    in_specs = (
        P(None, "ep"),
        P("ep"),
        P("ep", "tp"),
        P("ep", "tp"),
        P("ep", "tp"),
        P("tp"),
        P("ep", None, "tp", None),
        P("ep", None, "tp", None),
        P("ep"),
        P("tp", "ep"),
        P("tp"),
        P("ep"),
        P(),
        P(),
        P("ep", None, "tp"),
        P("ep", None, "tp"),
        P("ep", "tp", None),
        P("ep", "tp"),
        P("ep", "tp"),
        P("tp", "ep"),
        P("ep"),
    )
    out_specs = (P(None, "ep"), P("ep", "tp"), P("ep", "tp"))
    return jax.shard_map(
        per_device, mesh=mesh, in_specs=in_specs, out_specs=out_specs, check_vma=False
    )
```
